256 devices in a mesh: grp: 2 (over y), sp: 16 (over z), fs: 4 (over x), tp: 2 (over core).
Axes of the slice: x: 4, y: 2, z: 16, core: 2. Of those that a mesh axis runs over, the one named last changes fastest.
The devices are a block of a 4x16x16 slice.
Arguments:
- tokens: bfloat16 [4, 24576, 2048], P('fs', ('grp', 'sp'), 'tp'), parts along dimension 1, may hold values from -12 to 12
- norm_gain: float32 [2048], replicated, may hold values from 0.1 to 1.9
- query_weight: bfloat16 [2048, 16, 64], P(None, 'tp'), may hold values from -3 to 3
- key_weight: bfloat16 [2048, 4, 64], P(None, 'tp'), may hold values from -3 to 3
- value_weight: bfloat16 [2048, 4, 64], P(None, 'tp'), may hold values from -0.125 to 0.125
- sink_logit: float32 [16], P('tp'), may hold values from 1 to 6
- pool_weight: bfloat16 [2048, 4, 256], P(None, None, 'tp'), may hold values from -0.125 to 0.125
- attn_out_weight: bfloat16 [16, 64, 2048], P('tp'), may hold values from -0.5 to 0.5
- pool_out_weight: bfloat16 [4, 256, 2048], P(None, 'tp'), may hold values from -0.1875 to 0.1875
Outputs:
- mixed: bfloat16 [4, 24576, 2048], P('fs', ('grp', 'sp', 'tp')), parts along dimension 1
The draws below stay inside these ranges and needn't reach their ends.
There are 2 independent parts, one for each index of `grp`. The reference program is written for one: setup_inputs(seed, part) draws one part's arguments, and reference() takes and returns one part's arrays. A program takes and returns all parts, laid end to end along the dimension named above; an argument that names none is the same for every part. Nothing has to cross between parts.
All inputs are finite; a program needn't handle non-finite values.
Results may differ from the reference program's by a relative error of at most 0.0095.
The reference program's roundings to bfloat16 on the way (of `normed`, `weight`, `attended` and `pooled`) count: a program that leaves them out, or rounds other values in their place, can miss the bound.
Values may be sent and summed in bfloat16 or wider, within the bound.
A program may use at most 128 MiB of HBM per device.

```python
import jax
import jax.numpy as jnp
from jax import lax

D = 2048
HEADS = 16
KV_HEADS = 4
HEAD_DIM = 64
POOL_CH = 256
WINDOW = 128
TOK_DEV = 768
SEQS = 4
LEN = 12288


def draw_tokens(key, part):
    first, second, third = jax.random.split(jax.random.fold_in(key, 11), 3)
    blocks = LEN // TOK_DEV
    base = jax.random.normal(first, (SEQS, blocks, TOK_DEV, D), jnp.float32)
    offset = jax.random.normal(second, (SEQS, 1, 1, D), jnp.float32)
    factor = jax.random.uniform(third, (SEQS, blocks, 1, 1), jnp.float32, -1.5, 1.5)
    values = jnp.clip(base + factor * offset, -12.0, 12.0)
    return values.reshape(SEQS, LEN, D).astype(jnp.bfloat16)


def projection(key, heads):
    values = jax.random.normal(key, (D, heads, HEAD_DIM), jnp.float32) * D ** (-0.5)
    return jnp.clip(values, -3.0, 3.0).astype(jnp.bfloat16)


def draw_query_weight(key, part):
    return projection(jax.random.fold_in(key, 21), HEADS)


def draw_key_weight(key, part):
    return projection(jax.random.fold_in(key, 31), KV_HEADS)


def block_levels(stream_key, extent, shards, low, top_value):
    def one(dim, blocks):
        heights = jax.random.uniform(jax.random.fold_in(jax.random.fold_in(stream_key, 6), dim), (blocks,), jnp.float32, low / len(shards), top_value / len(shards))
        return jnp.repeat(jnp.exp(heights), extent[dim] // blocks).reshape((-1,) + (1,) * (len(extent) - dim - 1))

    level = one(*shards[0])
    for cut in shards[1:]:
        level = level * one(*cut)
    return level


def noise(own_key, extent, deviation, limit, cuts=(), kind=jnp.bfloat16):
    loudness = block_levels(own_key, extent, cuts, -0.22, 0.18) if cuts else 1.0
    values = jax.random.normal(own_key, extent, jnp.float32) * deviation * loudness
    return jnp.minimum(jnp.maximum(values, -limit), limit).astype(kind)


def setup_inputs(seed: int = 0, part: int = 0) -> dict:
    streams_of = jax.random.split(jax.random.key(seed), 10)
    part_splits = jax.random.split(jax.random.fold_in(streams_of[9], part), 10)
    tokens = draw_tokens(jax.random.fold_in(jax.random.fold_in(streams_of[9], part), 71), part)
    norm_gain = jnp.clip(1.0 + 0.18 * jax.random.normal(streams_of[1], (D,), jnp.float32), 0.1, 1.9)
    query_weight = draw_query_weight(jax.random.fold_in(streams_of[9], 71), part)
    key_weight = draw_key_weight(jax.random.fold_in(streams_of[9], 71), part)
    value_weight = noise(streams_of[4], (D, KV_HEADS, HEAD_DIM), D ** -0.5, 0.125, ((1, 2),))
    sink_logit = jnp.clip(1.0 + 5.0 * jax.random.uniform(streams_of[5], (HEADS,), jnp.float32) ** block_levels(streams_of[5], (HEADS,), ((0, 2),), -0.2, 0.2), 1.0, 6.0)
    pool_weight = noise(streams_of[6], (D, 4, POOL_CH), D ** -0.5, 0.125, ((2, 2),))
    attn_out_weight = noise(streams_of[7], (HEADS, HEAD_DIM, D), (HEADS * HEAD_DIM // 8) ** -0.5, 0.5, ((0, 2),))
    pool_out_weight = noise(streams_of[8], (4, POOL_CH, D), (4 * POOL_CH) ** -0.5, 0.1875, ((1, 2),))
    return dict(tokens=tokens, norm_gain=norm_gain, query_weight=query_weight, key_weight=key_weight, value_weight=value_weight, sink_logit=sink_logit, pool_weight=pool_weight, attn_out_weight=attn_out_weight, pool_out_weight=pool_out_weight)


def rms_norm(rows, gain):
    values = rows.astype(jnp.float32)
    scale = lax.rsqrt(lax.optimization_barrier(jnp.mean(values * values, axis=-1, keepdims=True)) + 1e-06)
    return (values * scale * gain).astype(jnp.bfloat16)

def attend(query, key, value, sinks):
    group = HEADS // KV_HEADS
    blocks = LEN // WINDOW
    qb = query.reshape(blocks, WINDOW, KV_HEADS, group, HEAD_DIM).astype(jnp.float32)

    def banded(tensor):
        tb = tensor.reshape(blocks, WINDOW, KV_HEADS, HEAD_DIM)
        before = jnp.concatenate([jnp.zeros_like(tb[:1]), tb[:-1]], axis=0)
        return jnp.concatenate([before, tb], axis=1).astype(jnp.float32)
    kw = banded(key)
    vw = banded(value)
    qi = jnp.arange(WINDOW, dtype=jnp.int32)[:, None]
    kj = jnp.arange(2 * WINDOW, dtype=jnp.int32)[None, :]
    dist = WINDOW + qi - kj
    inside = (dist >= 0) & (dist < WINDOW)
    key_pos = jnp.arange(blocks, dtype=jnp.int32)[:, None, None] * WINDOW - WINDOW + kj[None]
    mask = inside[None] & (key_pos >= 0)
    scores = jnp.einsum('nqhgd,nkhd->nhgqk', qb, kw) * HEAD_DIM ** (-0.5)
    scores = jnp.where(mask[:, None, None], scores, -jnp.inf)
    sink = sinks.reshape(1, KV_HEADS, group, 1, 1)
    top = jnp.maximum(lax.optimization_barrier(jnp.max(scores, axis=-1, keepdims=True)), sink)
    expo = jnp.exp(scores - top)
    total = lax.optimization_barrier(jnp.sum(expo, axis=-1, keepdims=True)) + jnp.exp(sink - top)
    weight = (expo / total).astype(jnp.bfloat16)
    out = jnp.einsum('nhgqk,nkhd->nqhgd', weight.astype(jnp.float32), vw)
    return out.reshape(LEN, HEADS * HEAD_DIM).astype(jnp.bfloat16)

def pool(pooled_in):
    values = pooled_in.astype(jnp.float32)
    sums = jnp.cumsum(values, axis=0)
    count = jnp.arange(1, LEN + 1).astype(jnp.float32)[:, None]
    parts = []
    for group, reach in enumerate((2, 4, 16)):
        col = sums[:, group]
        lower = jnp.concatenate([jnp.zeros((reach, POOL_CH), jnp.float32), col[:-reach]], axis=0)
        parts.append((col - lower) / jnp.minimum(count, float(reach)))
    parts.append(sums[:, 3] / count)
    mean = jnp.stack(parts, axis=1)
    return (mean - values).astype(jnp.bfloat16)

def one_sequence(rows, norm_gain, query_weight, key_weight, value_weight, sink_logit, pool_weight, attn_out_weight, pool_out_weight):
    normed = rms_norm(rows, norm_gain)
    query = jnp.dot(normed, query_weight.reshape(D, -1), preferred_element_type=jnp.float32).astype(jnp.bfloat16)
    key = jnp.dot(normed, key_weight.reshape(D, -1), preferred_element_type=jnp.float32).astype(jnp.bfloat16)
    value = jnp.dot(normed, value_weight.reshape(D, -1), preferred_element_type=jnp.float32).astype(jnp.bfloat16)
    pooled_in = jnp.dot(normed, pool_weight.reshape(D, -1), preferred_element_type=jnp.float32).astype(jnp.bfloat16)
    attended = attend(query, key, value, sink_logit)
    pooled = pool(pooled_in.reshape(LEN, 4, POOL_CH)).reshape(LEN, 4 * POOL_CH)
    total = jnp.dot(attended, attn_out_weight.reshape(-1, D), preferred_element_type=jnp.float32)
    total = total + jnp.dot(pooled, pool_out_weight.reshape(-1, D), preferred_element_type=jnp.float32)
    return total.astype(jnp.bfloat16)

def reference(tokens, norm_gain, query_weight, key_weight, value_weight, sink_logit, pool_weight, attn_out_weight, pool_out_weight):

    def apply(rows):
        return one_sequence(rows, norm_gain, query_weight, key_weight, value_weight, sink_logit, pool_weight, attn_out_weight, pool_out_weight)
    return lax.map(apply, tokens)
```

```python
import functools

import jax
import jax.numpy as jnp
from jax import lax
from jax.experimental import pallas as pl
from jax.experimental.pallas import tpu as pltpu
from jax.sharding import PartitionSpec as P

WINDOW = 128
REACHES = (2, 4, 16)
TAIL = 16
GROUP = 4
CHUNKS = 3
OUT_CHUNKS = 4
NEG = -1e30
BF16 = jnp.bfloat16
F32 = jnp.float32
MESH = pl.DeviceIdType.MESH
NT = (((1,), (1,)), ((), ()))


def kernel(
    tok_hbm, gain_ref, wq_hbm, wk_hbm, wv_hbm, sink_ref, wp_hbm, wa_hbm, wpo_hbm,
    out_hbm,
    tok, nrm, wqkv, wpraw, wp, wo, qt, kx, vt, px, att, l3, bt,
    kin, vin, pin, ktail, vtail, ptail, totout, totin, carryout, carryin,
    own, sendbuf, recvbuf, outbuf,
    tok_sem, w_sem, tsend, trecv, tail_send, tail_recv, tot_send, tot_recv,
    carry_send, carry_recv, out_send, out_recv, out_sem, ready,
):
    me = lax.axis_index("tp")
    other = 1 - me
    z = lax.axis_index("sp")
    nz = lax.axis_size("sp")
    rows, width = nrm.shape
    half = width // 2
    heads = qt.shape[0] // 64
    kv = kx.shape[1] // 64
    group = heads // kv
    nb = rows // WINDOW
    crow = rows // CHUNKS
    gi = lax.rem(z, GROUP)
    base = z - gi

    def tok_copy(c):
        return pltpu.make_async_copy(
            tok_hbm.at[0, pl.ds(c * crow, crow), :],
            tok.at[pl.ds(c * crow, crow), pl.ds(pl.multiple_of(me * half, half), half)],
            tok_sem.at[c],
        )

    qn, kn = wq_hbm.shape[0], wk_hbm.shape[0]
    loads = [
        pltpu.make_async_copy(wp_hbm, wpraw, w_sem.at[0]),
        pltpu.make_async_copy(wq_hbm, wqkv.at[pl.ds(0, qn)], w_sem.at[1]),
        pltpu.make_async_copy(wk_hbm, wqkv.at[pl.ds(qn, kn)], w_sem.at[2]),
        pltpu.make_async_copy(wv_hbm, wqkv.at[pl.ds(qn + kn, kn)], w_sem.at[3]),
        pltpu.make_async_copy(wa_hbm, wo.at[pl.ds(0, qn)], w_sem.at[4]),
        pltpu.make_async_copy(wpo_hbm, wo.at[pl.ds(qn, wo.shape[0] - qn)], w_sem.at[5]),
    ]
    for c in range(CHUNKS):
        tok_copy(c).start()
    for load in loads:
        load.start()

    barrier = pltpu.get_barrier_semaphore()
    pl.semaphore_signal(barrier, inc=1, device_id={"tp": other}, device_id_type=MESH)

    def sends_to(d):
        inside = gi + d < GROUP
        leads = gi == GROUP - 1
        return (inside | leads) & (z + d < nz) if d < GROUP else leads & (z + d < nz)

    def hears_from(d):
        return (d <= gi) | ((d == gi + 1) & (base > 0))

    for d in range(1, GROUP + 1):

        @pl.when(sends_to(d))
        def _():
            pl.semaphore_signal(barrier, inc=1, device_id={"sp": z + d}, device_id_type=MESH)

    behind = gi + jnp.where(base > 0, 1, 0)
    pl.semaphore_wait(barrier, 1 + behind)
    for d in range(1, GROUP + 1):

        @pl.when(hears_from(d))
        def _():
            pl.semaphore_signal(ready.at[d - 1], inc=1, device_id={"sp": z - d}, device_id_type=MESH)

    def tok_send(c):
        return pltpu.make_async_remote_copy(
            src_ref=tok_hbm.at[0, pl.ds(c * crow, crow), :],
            dst_ref=tok.at[pl.ds(c * crow, crow), pl.ds(pl.multiple_of(me * half, half), half)],
            send_sem=tsend.at[c],
            recv_sem=trecv.at[c],
            device_id={"tp": other},
            device_id_type=MESH,
        )

    for c in range(CHUNKS):
        tok_send(c).start()

    loads[0].wait()
    pi = lax.broadcasted_iota(jnp.int32, (256, 256), 0)
    pc = lax.broadcasted_iota(jnp.int32, (256, 256), 1)
    perm = jnp.where(pc == 4 * (pi & 63) + (pi >> 6), 1.0, 0.0).astype(BF16)

    def sort_step(r, _):
        at = pl.multiple_of(r * 512, 512)
        pair = jnp.concatenate(
            [wpraw[pl.ds(at, 256), :], wpraw[pl.ds(at + 256, 256), :]], axis=1
        )
        got = jnp.dot(perm, pair, preferred_element_type=F32).astype(BF16)
        to = pl.multiple_of(r * 128, 128)
        for g in range(4):
            for s in range(2):
                wp[pl.ds(to + 64 * s, 64), pl.ds(128 * g, 128)] = got[
                    64 * g : 64 * g + 64, 128 * s : 128 * s + 128
                ]
        return _

    lax.fori_loop(0, width // 128, sort_step, 0)

    gain = gain_ref[...]
    for load in loads[1:4]:
        load.wait()

    def norm_step(r, _):
        at = pl.multiple_of(r * 16, 16)
        x = tok[pl.ds(at, 16), :].astype(F32)
        scale = lax.rsqrt(jnp.sum(x * x, axis=1, keepdims=True) * (1.0 / width) + 1e-06)
        nrm[pl.ds(at, 16), :] = (x * scale * gain).astype(BF16)
        return _

    for c in range(CHUNKS):
        tok_copy(c).wait()
        tok_send(c).wait_recv()
        lax.fori_loop(c * crow // 16, (c + 1) * crow // 16, norm_step, 0)
        lo = c * crow
        part = nrm[lo : lo + crow, :]
        pooled_in = jnp.dot(part, wp[...], preferred_element_type=F32).astype(BF16)
        px[WINDOW + lo : WINDOW + lo + crow, :] = pooled_in
        for b in range(crow // WINDOW):
            piece = pooled_in[b * WINDOW : (b + 1) * WINDOW, 384:].astype(F32)
            n = c * (crow // WINDOW) + b
            bt[n : n + 1, :] = jnp.sum(piece, axis=0, keepdims=True)
        qkv = lax.dot_general(wqkv[...], part, NT, preferred_element_type=F32)
        qt[:, lo : lo + crow] = (qkv[:qn] * 0.125).astype(BF16)
        kx[WINDOW + lo : WINDOW + lo + crow, :] = jnp.transpose(qkv[qn : qn + kn]).astype(BF16)
        vt[:, WINDOW + lo : WINDOW + lo + crow] = qkv[qn + kn :].astype(BF16)

    total = jnp.sum(bt[0:nb, :], axis=0, keepdims=True)
    totout[...] = jnp.broadcast_to(total, totout.shape)
    ktail[...] = kx[rows : rows + WINDOW, :]
    vtail[...] = vt[:, rows : rows + WINDOW]
    ptail[...] = px[WINDOW + rows - TAIL : WINDOW + rows, 0:384]

    def tail_copy(n):
        src, dst = ((ktail, kin), (vtail, vin), (ptail, pin))[n]
        return pltpu.make_async_remote_copy(
            src_ref=src,
            dst_ref=dst,
            send_sem=tail_send.at[n],
            recv_sem=tail_recv.at[n],
            device_id={"sp": z + 1},
            device_id_type=MESH,
        )

    def tot_copy(d):
        return pltpu.make_async_remote_copy(
            src_ref=totout,
            dst_ref=totin.at[d - 1],
            send_sem=tot_send.at[d - 1],
            recv_sem=tot_recv.at[d - 1],
            device_id={"sp": z + d},
            device_id_type=MESH,
        )

    def carry_copy(d):
        return pltpu.make_async_remote_copy(
            src_ref=carryout,
            dst_ref=carryin,
            send_sem=carry_send.at[d - 1],
            recv_sem=carry_recv,
            device_id={"sp": z + d},
            device_id_type=MESH,
        )

    leads = (gi == GROUP - 1) & (z + 1 < nz)
    for d in range(1, GROUP):

        @pl.when(gi + d < GROUP)
        def _():
            pl.semaphore_wait(ready.at[d - 1], 1)
            tot_copy(d).start()

    @pl.when(leads)
    def _():
        pl.semaphore_wait(ready.at[0], 1)

    @pl.when(z + 1 < nz)
    def _():
        for n in range(3):
            tail_copy(n).start()

    keyi = lax.broadcasted_iota(jnp.int32, (WINDOW, group * WINDOW), 0)
    posi = lax.broadcasted_iota(jnp.int32, (WINDOW, group * WINDOW), 1) & (WINDOW - 1)
    bi = lax.broadcasted_iota(jnp.int32, (WINDOW, 2 * WINDOW), 0)
    bj = lax.broadcasted_iota(jnp.int32, (WINDOW, 2 * WINDOW), 1)
    gap = bi + WINDOW - bj
    bands = [jnp.where((gap >= 0) & (gap < r), 1.0, 0.0).astype(BF16) for r in REACHES]
    bands.append(jnp.where((gap >= 0) & (bj >= WINDOW), 1.0, 0.0).astype(BF16))

    def counts(b):
        first = z * rows + b * WINDOW + 1
        return (lax.broadcasted_iota(jnp.int32, (WINDOW, 1), 0) + first).astype(F32)

    def block(b, first):
        at = b * WINDOW if first else pl.multiple_of(b * WINDOW, WINDOW)
        here = keyi <= posi
        for h in range(kv):
            keys = kx[pl.ds(at, 2 * WINDOW), :]
            qs = jnp.concatenate(
                [
                    qt[64 * (group * h + j) : 64 * (group * h + j + 1), pl.ds(at, WINDOW)]
                    for j in range(group)
                ],
                axis=1,
            )
            blank = jnp.zeros_like(qs)
            qpad = jnp.concatenate([qs if n == h else blank for n in range(kv)], axis=0)
            s = jnp.dot(keys, qpad, preferred_element_type=F32)
            before = s[:WINDOW]
            if first:
                before = before + jnp.where(z > 0, 0.0, NEG)
            s = jnp.where(here, s[WINDOW:], before)
            sink = jnp.concatenate(
                [jnp.full((1, WINDOW), sink_ref[group * h + j], F32) for j in range(group)], axis=1
            )
            top = jnp.maximum(jnp.max(s, axis=0, keepdims=True), sink)
            e = jnp.exp(s - top)
            tot = jnp.sum(e, axis=0, keepdims=True) + jnp.exp(sink - top)
            w = e * (1.0 / tot)
            wt = jnp.concatenate(
                [jnp.where(here, 0.0, w).astype(BF16), jnp.where(here, w, 0.0).astype(BF16)],
                axis=0,
            )
            o = jnp.dot(
                vt[64 * h : 64 * (h + 1), pl.ds(at, 2 * WINDOW)], wt, preferred_element_type=F32
            )
            o = jnp.concatenate(
                [o[:, j * WINDOW : (j + 1) * WINDOW] for j in range(group)], axis=0
            )
            att[pl.ds(at, WINDOW), 64 * group * h : 64 * group * (h + 1)] = jnp.transpose(
                o
            ).astype(BF16)
        count = counts(b)
        for g in range(3):
            near = px[pl.ds(at, 2 * WINDOW), 128 * g : 128 * (g + 1)]
            sums = jnp.dot(bands[g], near, preferred_element_type=F32)
            mean = sums * (1.0 / jnp.minimum(count, float(REACHES[g])))
            att[pl.ds(at, WINDOW), qn + 128 * g : qn + 128 * (g + 1)] = (
                mean - near[WINDOW:].astype(F32)
            ).astype(BF16)
        near = px[pl.ds(at, 2 * WINDOW), 384:512]
        l3[pl.ds(at, WINDOW), :] = jnp.dot(bands[3], near, preferred_element_type=F32)

    px[0:WINDOW, :] = jnp.zeros((WINDOW, px.shape[1]), BF16)
    kx[0:WINDOW, :] = jnp.zeros((WINDOW, kx.shape[1]), BF16)
    vt[:, 0:WINDOW] = jnp.zeros((vt.shape[0], WINDOW), BF16)

    def block_step(i, _):
        block(nb - 1 - i, False)
        return _

    lax.fori_loop(0, nb - 1, block_step, 0)

    @pl.when(z > 0)
    def _():
        for n in range(3):
            tail_copy(n).wait_recv()
        kx[0:WINDOW, :] = kin[...]
        vt[:, 0:WINDOW] = vin[...]
        px[WINDOW - TAIL : WINDOW, 0:384] = pin[...]

    block(0, True)

    for d in range(1, GROUP):

        @pl.when(d <= gi)
        def _():
            tot_copy(d).wait_recv()

        @pl.when(d > gi)
        def _():
            totin[d - 1] = jnp.zeros(totin.shape[1:], F32)

    @pl.when(base > 0)
    def _():
        carry_copy(1).wait_recv()

    @pl.when(base == 0)
    def _():
        carryin[...] = jnp.zeros(carryin.shape, F32)

    carried = carryin[...]
    for d in range(1, GROUP):
        carried = carried + totin[d - 1]

    @pl.when(leads)
    def _():
        carryout[...] = carried + totout[...]
        for d in range(1, GROUP + 1):
            if d > 1:
                pl.semaphore_wait(ready.at[d - 1], 1)
            carry_copy(d).start()

    run = carried[0:1, :]
    for b in range(nb):
        lo = b * WINDOW
        mean = (l3[lo : lo + WINDOW, :] + run) * (1.0 / counts(b))
        run = run + bt[b : b + 1, :]
        att[lo : lo + WINDOW, qn + 384 :] = (
            mean - px[WINDOW + lo : WINDOW + lo + WINDOW, 384:].astype(F32)
        ).astype(BF16)

    orow = rows // 2
    ocol = width // OUT_CHUNKS
    for load in loads[4:]:
        load.wait()

    def out_copy(n):
        cols = pl.ds(n * ocol, ocol)
        return pltpu.make_async_remote_copy(
            src_ref=sendbuf.at[:, cols],
            dst_ref=recvbuf.at[:, cols],
            send_sem=out_send.at[n],
            recv_sem=out_recv.at[n],
            device_id={"tp": other},
            device_id_type=MESH,
        )

    def out_store(n):
        cols = pl.ds(n * ocol, ocol)
        return pltpu.make_async_copy(outbuf.at[:, cols], out_hbm.at[:, cols], out_sem.at[n])

    theirs = pl.ds(pl.multiple_of(other * orow, orow), orow)
    ours = pl.ds(pl.multiple_of(me * orow, orow), orow)
    for n in range(OUT_CHUNKS):
        cols = slice(n * ocol, (n + 1) * ocol)
        sendbuf[:, cols] = jnp.dot(
            att[theirs, :], wo[:, cols], preferred_element_type=F32
        ).astype(BF16)
        out_copy(n).start()
    for n in range(OUT_CHUNKS):
        cols = slice(n * ocol, (n + 1) * ocol)
        own[...] = jnp.dot(att[ours, :], wo[:, cols], preferred_element_type=F32)
        out_copy(n).wait_recv()
        outbuf[:, cols] = (own[...] + recvbuf[:, cols].astype(F32)).astype(BF16)
        out_store(n).start()

    for c in range(CHUNKS):
        tok_send(c).wait_send()
    for d in range(1, GROUP):

        @pl.when(gi + d < GROUP)
        def _():
            tot_copy(d).wait_send()

    @pl.when(z + 1 < nz)
    def _():
        for n in range(3):
            tail_copy(n).wait_send()

    @pl.when(leads)
    def _():
        for d in range(1, GROUP + 1):
            carry_copy(d).wait_send()

    for n in range(OUT_CHUNKS):
        out_copy(n).wait_send()
        out_store(n).wait()


def shards(
    tokens,
    norm_gain,
    query_weight,
    key_weight,
    value_weight,
    sink_logit,
    pool_weight,
    attn_out_weight,
    pool_out_weight,
):
    rows, half = tokens.shape[1:]
    width = 2 * half
    assert lax.axis_size("tp") == 2 and lax.axis_size("sp") % GROUP == 0
    turned = [
        jnp.transpose(w, (1, 2, 0)).reshape(-1, width)
        for w in (query_weight, key_weight, value_weight)
    ]
    qn, kn = turned[0].shape[0], turned[1].shape[0]
    pn = pool_weight.shape[1] * pool_weight.shape[2]
    wp = pool_weight.reshape(-1, pool_weight.shape[2])
    wa = attn_out_weight.reshape(-1, width)
    wpo = pool_out_weight.reshape(-1, width)
    anyspace = pl.BlockSpec(memory_space=pl.ANY)
    vm = pltpu.VMEM
    dma = pltpu.SemaphoreType.DMA
    orow = rows // 2
    out = pl.pallas_call(
        kernel,
        out_shape=jax.ShapeDtypeStruct((orow, width), BF16),
        in_specs=[
            anyspace,
            pl.BlockSpec(memory_space=pltpu.VMEM),
            anyspace,
            anyspace,
            anyspace,
            pl.BlockSpec(memory_space=pltpu.SMEM),
            anyspace,
            anyspace,
            anyspace,
        ],
        out_specs=anyspace,
        scratch_shapes=[
            vm((rows, width), BF16),
            vm((rows, width), BF16),
            vm((qn + 2 * kn, width), BF16),
            vm(wp.shape, BF16),
            vm((width, pn), BF16),
            vm((qn + pn, width), BF16),
            vm((qn, rows), BF16),
            vm((WINDOW + rows, kn), BF16),
            vm((kn, WINDOW + rows), BF16),
            vm((WINDOW + rows, pn), BF16),
            vm((rows, qn + pn), BF16),
            vm((rows, 128), F32),
            vm((8, 128), F32),
            vm((WINDOW, kn), BF16),
            vm((kn, WINDOW), BF16),
            vm((TAIL, 384), BF16),
            vm((WINDOW, kn), BF16),
            vm((kn, WINDOW), BF16),
            vm((TAIL, 384), BF16),
            vm((8, 128), F32),
            vm((GROUP - 1, 8, 128), F32),
            vm((8, 128), F32),
            vm((8, 128), F32),
            vm((orow, width // OUT_CHUNKS), F32),
            vm((orow, width), BF16),
            vm((orow, width), BF16),
            vm((orow, width), BF16),
            dma((CHUNKS,)),
            dma((6,)),
            dma((CHUNKS,)),
            dma((CHUNKS,)),
            dma((3,)),
            dma((3,)),
            dma((GROUP - 1,)),
            dma((GROUP - 1,)),
            dma((GROUP,)),
            dma(()),
            dma((OUT_CHUNKS,)),
            dma((OUT_CHUNKS,)),
            dma((OUT_CHUNKS,)),
            pltpu.SemaphoreType.REGULAR((GROUP,)),
        ],
        compiler_params=pltpu.CompilerParams(
            collective_id=0, has_side_effects=True, vmem_limit_bytes=60 * 1024 * 1024
        ),
    )(tokens, norm_gain.reshape(1, width), *turned, sink_logit, wp, wa, wpo)
    return out[None]


def solution(mesh):
    in_specs = (
        P("fs", ("grp", "sp"), "tp"),
        P(),
        P(None, "tp", None),
        P(None, "tp", None),
        P(None, "tp", None),
        P("tp"),
        P(None, None, "tp"),
        P("tp", None, None),
        P(None, "tp", None),
    )
    out_specs = P("fs", ("grp", "sp", "tp"), None)
    return jax.shard_map(shards, mesh=mesh, in_specs=in_specs, out_specs=out_specs, check_vma=False)
```

```python
import functools

import jax
import jax.numpy as jnp
from jax import lax
from jax.experimental import pallas as pl
from jax.experimental.pallas import tpu as pltpu
from jax.sharding import PartitionSpec as P

WINDOW = 128
REACHES = (2, 4, 16)
TAIL = 16
GROUP = 4
CHUNKS = 3
OUT_CHUNKS = 2
NEG = -1e30
BF16 = jnp.bfloat16
F32 = jnp.float32
MESH = pl.DeviceIdType.MESH
NT = (((1,), (1,)), ((), ()))


def kernel(
    tok_hbm, gain_hbm, wq_hbm, wk_hbm, wv_hbm, sink_hbm, wp_hbm, wa_hbm, wpo_hbm,
    outbuf,
    tok, nrm0, nrm1, nrm2, gain_ref, sink_ref, wqkv, wpraw, wp, wo, qt, kx, vt, px, att, l3, bt,
    sbuf, pbuf,
    kin, vin, pin, ktail, vtail, ptail, totout, totin, carryout, carryin,
    sendbuf, recvbuf,
    tok_sem, w_sem, tsend, trecv, tail_send, tail_recv, tot_send, tot_recv,
    carry_send, carry_recv, out_send, out_recv, ready,
):
    me = lax.axis_index("tp")
    other = 1 - me
    z = lax.axis_index("sp")
    nz = lax.axis_size("sp")
    rows, width = tok.shape
    nrm = (nrm0, nrm1, nrm2)
    half = width // 2
    heads = qt.shape[0] // 64
    kv = kx.shape[1] // 64
    group = heads // kv
    nb = rows // WINDOW
    crow = rows // CHUNKS
    gi = lax.rem(z, GROUP)
    base = z - gi

    def tok_copy(c):
        return pltpu.make_async_copy(
            tok_hbm.at[0, pl.ds(c * crow, crow), :],
            tok.at[pl.ds(c * crow, crow), pl.ds(pl.multiple_of(me * half, half), half)],
            tok_sem.at[c],
        )

    qn, kn = wq_hbm.shape[0], wk_hbm.shape[0]
    loads = [
        pltpu.make_async_copy(wp_hbm, wpraw, w_sem.at[0]),
        pltpu.make_async_copy(wq_hbm, wqkv.at[pl.ds(0, qn)], w_sem.at[1]),
        pltpu.make_async_copy(wk_hbm, wqkv.at[pl.ds(qn, kn)], w_sem.at[2]),
        pltpu.make_async_copy(wv_hbm, wqkv.at[pl.ds(qn + kn, kn)], w_sem.at[3]),
        pltpu.make_async_copy(wa_hbm, wo.at[pl.ds(0, qn)], w_sem.at[4]),
        pltpu.make_async_copy(wpo_hbm, wo.at[pl.ds(qn, wo.shape[0] - qn)], w_sem.at[5]),
        pltpu.make_async_copy(gain_hbm, gain_ref, w_sem.at[6]),
        pltpu.make_async_copy(sink_hbm, sink_ref, w_sem.at[7]),
    ]
    barrier = pltpu.get_barrier_semaphore()
    pl.semaphore_signal(barrier, inc=1, device_id={"tp": other}, device_id_type=MESH)
    for c in range(CHUNKS):
        tok_copy(c).start()
    for load in (*loads[6:], *loads[:6]):
        load.start()

    def sends_to(d):
        inside = gi + d < GROUP
        leads = gi == GROUP - 1
        return (inside | leads) & (z + d < nz) if d < GROUP else leads & (z + d < nz)

    def hears_from(d):
        return (d <= gi) | ((d == gi + 1) & (base > 0))

    for d in range(1, GROUP + 1):

        @pl.when(sends_to(d))
        def _():
            pl.semaphore_signal(barrier, inc=1, device_id={"sp": z + d}, device_id_type=MESH)

    behind = gi + jnp.where(base > 0, 1, 0)
    pl.semaphore_wait(barrier, 1 + behind)

    def tok_send(c):
        return pltpu.make_async_remote_copy(
            src_ref=tok_hbm.at[0, pl.ds(c * crow, crow), :],
            dst_ref=tok.at[pl.ds(c * crow, crow), pl.ds(pl.multiple_of(me * half, half), half)],
            send_sem=tsend.at[c],
            recv_sem=trecv.at[c],
            device_id={"tp": other},
            device_id_type=MESH,
        )

    for c in range(CHUNKS):
        tok_send(c).start()
    for d in range(1, GROUP + 1):

        @pl.when(hears_from(d))
        def _():
            pl.semaphore_signal(ready.at[d - 1], inc=1, device_id={"sp": z - d}, device_id_type=MESH)

    loads[0].wait()
    pi = lax.broadcasted_iota(jnp.int32, (256, 256), 0)
    pc = lax.broadcasted_iota(jnp.int32, (256, 256), 1)
    perm = jnp.where(pc == 4 * (pi & 63) + (pi >> 6), 1.0, 0.0).astype(BF16)

    def sort_one(r):
        at = pl.multiple_of(r * 512, 512)
        pair = jnp.concatenate(
            [wpraw[pl.ds(at, 256), :], wpraw[pl.ds(at + 256, 256), :]], axis=1
        )
        got = jnp.dot(perm, pair, preferred_element_type=F32).astype(BF16)
        to = pl.multiple_of(r * 128, 128)
        for g in range(4):
            for s in range(2):
                wp[pl.ds(to + 64 * s, 64), pl.ds(128 * g, 128)] = got[
                    64 * g : 64 * g + 64, 128 * s : 128 * s + 128
                ]

    def sort_step(r, _):
        for n in range(4):
            sort_one(4 * r + n)
        return _

    lax.fori_loop(0, width // 512, sort_step, 0)

    for load in (*loads[1:4], *loads[6:]):
        load.wait()
    gain = gain_ref[...]

    def norm(c):
        for n in range(crow // 16):
            x = tok[c * crow + 16 * n : c * crow + 16 * (n + 1), :].astype(F32)
            mean = jnp.sum(x * x, axis=1, keepdims=True) * (1.0 / width)
            scale = lax.rsqrt(mean + 1e-06)
            nrm[c][16 * n : 16 * (n + 1), :] = (x * scale * gain).astype(BF16)

    def project(c):
        lo = c * crow
        part = nrm[c][...]
        pooled_in = jnp.dot(part, wp[...], preferred_element_type=F32).astype(BF16)
        px[WINDOW + lo : WINDOW + lo + crow, :] = pooled_in
        for b in range(crow // WINDOW):
            piece = pooled_in[b * WINDOW : (b + 1) * WINDOW, 384:].astype(F32)
            n = c * (crow // WINDOW) + b
            bt[n : n + 1, :] = jnp.sum(piece, axis=0, keepdims=True)
        qkv = lax.dot_general(wqkv[...], part, NT, preferred_element_type=F32)
        qt[:, lo : lo + crow] = (qkv[:qn] * 0.125).astype(BF16)
        kx[WINDOW + lo : WINDOW + lo + crow, :] = jnp.transpose(qkv[qn : qn + kn]).astype(BF16)
        vt[:, WINDOW + lo : WINDOW + lo + crow] = qkv[qn + kn :].astype(BF16)

    tok_copy(0).wait()
    tok_send(0).wait_recv()
    norm(0)
    for c in range(1, CHUNKS):
        tok_copy(c).wait()
        tok_send(c).wait_recv()
    for c in range(CHUNKS):
        if c + 1 < CHUNKS:
            norm(c + 1)
        project(c)

    total = jnp.sum(bt[0:nb, :], axis=0, keepdims=True)
    totout[...] = jnp.broadcast_to(total, totout.shape)
    ktail[...] = kx[rows : rows + WINDOW, :]
    vtail[...] = vt[:, rows : rows + WINDOW]
    ptail[...] = px[WINDOW + rows - TAIL : WINDOW + rows, 0:384]

    def tail_copy(n):
        src, dst = ((ktail, kin), (vtail, vin), (ptail, pin))[n]
        return pltpu.make_async_remote_copy(
            src_ref=src,
            dst_ref=dst,
            send_sem=tail_send.at[n],
            recv_sem=tail_recv.at[n],
            device_id={"sp": z + 1},
            device_id_type=MESH,
        )

    def tot_copy(d):
        return pltpu.make_async_remote_copy(
            src_ref=totout,
            dst_ref=totin.at[d - 1],
            send_sem=tot_send.at[d - 1],
            recv_sem=tot_recv.at[d - 1],
            device_id={"sp": z + d},
            device_id_type=MESH,
        )

    def carry_copy(d):
        return pltpu.make_async_remote_copy(
            src_ref=carryout,
            dst_ref=carryin,
            send_sem=carry_send.at[d - 1],
            recv_sem=carry_recv,
            device_id={"sp": z + d},
            device_id_type=MESH,
        )

    leads = (gi == GROUP - 1) & (z + 1 < nz)
    for d in range(1, GROUP):

        @pl.when(gi + d < GROUP)
        def _():
            pl.semaphore_wait(ready.at[d - 1], 1)
            tot_copy(d).start()

    @pl.when(leads)
    def _():
        pl.semaphore_wait(ready.at[0], 1)

    @pl.when(z + 1 < nz)
    def _():
        for n in range(3):
            tail_copy(n).start()

    keyi = lax.broadcasted_iota(jnp.int32, (WINDOW, group * WINDOW), 0)
    posi = lax.broadcasted_iota(jnp.int32, (WINDOW, group * WINDOW), 1) & (WINDOW - 1)
    bi = lax.broadcasted_iota(jnp.int32, (WINDOW, 2 * WINDOW), 0)
    bj = lax.broadcasted_iota(jnp.int32, (WINDOW, 2 * WINDOW), 1)
    gap = bi + WINDOW - bj
    bands = [jnp.where((gap >= 0) & (gap < r), 1.0, 0.0).astype(BF16) for r in REACHES]
    bands.append(jnp.where((gap >= 0) & (bj >= WINDOW), 1.0, 0.0).astype(BF16))

    def counts(b):
        first = z * rows + b * WINDOW + 1
        return (lax.broadcasted_iota(jnp.int32, (WINDOW, 1), 0) + first).astype(F32)

    here = keyi <= posi
    quarter = here[:, :WINDOW]

    def scores(n, b, h):
        lo = b * WINDOW
        qs = jnp.concatenate(
            [
                qt[64 * (group * h + j) : 64 * (group * h + j + 1), lo : lo + WINDOW]
                for j in range(group)
            ],
            axis=1,
        )
        blank = jnp.zeros_like(qs)
        qpad = jnp.concatenate([qs if i == h else blank for i in range(kv)], axis=0)
        s = jnp.dot(kx[lo : lo + 2 * WINDOW, :], qpad, preferred_element_type=F32)
        before = s[:WINDOW]
        if b == 0:
            before = before + jnp.where(z > 0, 0.0, NEG)
        sbuf[n] = jnp.where(here, s[WINDOW:], before)

    def weights(n, b, h):
        for j in range(group):
            s = sbuf[n, :, j * WINDOW : (j + 1) * WINDOW]
            sink = jnp.full((1, WINDOW), sink_ref[group * h + j], F32)
            top = jnp.maximum(jnp.max(s, axis=0, keepdims=True), sink)
            e = jnp.exp(s - top)
            tot = jnp.sum(e, axis=0, keepdims=True) + jnp.exp(sink - top)
            pbuf[n, :, j * WINDOW : (j + 1) * WINDOW] = (e * (1.0 / tot)).astype(BF16)

    def attend(n, b, h):
        lo = b * WINDOW
        w = pbuf[n]
        blank = jnp.zeros_like(w)
        wt = jnp.concatenate([jnp.where(here, blank, w), jnp.where(here, w, blank)], axis=0)
        o = jnp.dot(
            vt[64 * h : 64 * (h + 1), lo : lo + 2 * WINDOW], wt, preferred_element_type=F32
        )
        o = jnp.concatenate([o[:, j * WINDOW : (j + 1) * WINDOW] for j in range(group)], axis=0)
        att[lo : lo + WINDOW, 64 * group * h : 64 * group * (h + 1)] = jnp.transpose(o).astype(BF16)

    def pool(b):
        lo = b * WINDOW
        count = counts(b)
        for g in range(3):
            near = px[lo : lo + 2 * WINDOW, 128 * g : 128 * (g + 1)]
            sums = jnp.dot(bands[g], near, preferred_element_type=F32)
            mean = sums * (1.0 / jnp.minimum(count, float(REACHES[g])))
            att[lo : lo + WINDOW, qn + 128 * g : qn + 128 * (g + 1)] = (
                mean - near[WINDOW:].astype(F32)
            ).astype(BF16)
        near = px[lo : lo + 2 * WINDOW, 384:512]
        l3[lo : lo + WINDOW, :] = jnp.dot(bands[3], near, preferred_element_type=F32)

    def blocks(which):
        chains = [(b, h) for b in which for h in range(kv)]
        last = len(chains)
        for n in range(last + 2):
            if n < last:
                scores(n, *chains[n])
            if 0 <= n - 1 < last:
                weights(n - 1, *chains[n - 1])
            if 0 <= n - 2 < last:
                attend(n - 2, *chains[n - 2])
                if chains[n - 2][1] == 0:
                    pool(chains[n - 2][0])

    px[0:WINDOW, :] = jnp.zeros((WINDOW, px.shape[1]), BF16)
    kx[0:WINDOW, :] = jnp.zeros((WINDOW, kx.shape[1]), BF16)
    vt[:, 0:WINDOW] = jnp.zeros((vt.shape[0], WINDOW), BF16)

    blocks(range(nb - 1, nb // 2 - 1, -1))

    @pl.when(z > 0)
    def _():
        for n in range(3):
            tail_copy(n).wait_recv()
        kx[0:WINDOW, :] = kin[...]
        vt[:, 0:WINDOW] = vin[...]
        px[WINDOW - TAIL : WINDOW, 0:384] = pin[...]

    blocks(range(nb // 2 - 1, -1, -1))

    for d in range(1, GROUP):

        @pl.when(d <= gi)
        def _():
            tot_copy(d).wait_recv()

        @pl.when(d > gi)
        def _():
            totin[d - 1] = jnp.zeros(totin.shape[1:], F32)

    @pl.when(base > 0)
    def _():
        carry_copy(1).wait_recv()

    @pl.when(base == 0)
    def _():
        carryin[...] = jnp.zeros(carryin.shape, F32)

    carried = carryin[...]
    for d in range(1, GROUP):
        carried = carried + totin[d - 1]

    @pl.when(leads)
    def _():
        carryout[...] = carried + totout[...]
        for d in range(1, GROUP + 1):
            if d > 1:
                pl.semaphore_wait(ready.at[d - 1], 1)
            carry_copy(d).start()

    run = carried[0:1, :]
    for b in range(nb):
        lo = b * WINDOW
        mean = (l3[lo : lo + WINDOW, :] + run) * (1.0 / counts(b))
        run = run + bt[b : b + 1, :]
        att[lo : lo + WINDOW, qn + 384 :] = (
            mean - px[WINDOW + lo : WINDOW + lo + WINDOW, 384:].astype(F32)
        ).astype(BF16)

    orow = rows // 2
    ocol = width // OUT_CHUNKS
    for load in loads[4:6]:
        load.wait()

    def out_copy(n):
        cols = pl.ds(n * ocol, ocol)
        return pltpu.make_async_remote_copy(
            src_ref=sendbuf.at[:, cols],
            dst_ref=recvbuf.at[:, cols],
            send_sem=out_send.at[n],
            recv_sem=out_recv.at[n],
            device_id={"tp": other},
            device_id_type=MESH,
        )

    theirs = pl.ds(pl.multiple_of(other * orow, orow), orow)
    ours = pl.ds(pl.multiple_of(me * orow, orow), orow)
    for n in range(OUT_CHUNKS):
        cols = slice(n * ocol, (n + 1) * ocol)
        sendbuf[:, cols] = jnp.dot(
            att[theirs, :], wo[:, cols], preferred_element_type=F32
        ).astype(BF16)
        out_copy(n).start()
    for n in range(OUT_CHUNKS):
        cols = slice(n * ocol, (n + 1) * ocol)
        out_copy(n).wait_recv()
        own = jnp.dot(att[ours, :], wo[:, cols], preferred_element_type=F32)
        outbuf[:, cols] = (own + recvbuf[:, cols].astype(F32)).astype(BF16)

    for c in range(CHUNKS):
        tok_send(c).wait_send()
    for d in range(1, GROUP):

        @pl.when(gi + d < GROUP)
        def _():
            tot_copy(d).wait_send()

    @pl.when(z + 1 < nz)
    def _():
        for n in range(3):
            tail_copy(n).wait_send()

    @pl.when(leads)
    def _():
        for d in range(1, GROUP + 1):
            carry_copy(d).wait_send()

    for n in range(OUT_CHUNKS):
        out_copy(n).wait_send()


def shards(
    tokens,
    norm_gain,
    query_weight,
    key_weight,
    value_weight,
    sink_logit,
    pool_weight,
    attn_out_weight,
    pool_out_weight,
):
    rows, half = tokens.shape[1:]
    width = 2 * half
    assert lax.axis_size("tp") == 2 and lax.axis_size("sp") % GROUP == 0
    turned = [
        jnp.transpose(w, (1, 2, 0)).reshape(-1, width)
        for w in (query_weight, key_weight, value_weight)
    ]
    qn, kn = turned[0].shape[0], turned[1].shape[0]
    pn = pool_weight.shape[1] * pool_weight.shape[2]
    wp = pool_weight.reshape(-1, pool_weight.shape[2])
    wa = attn_out_weight.reshape(-1, width)
    wpo = pool_out_weight.reshape(-1, width)
    anyspace = pl.BlockSpec(memory_space=pl.ANY)
    vm = pltpu.VMEM
    dma = pltpu.SemaphoreType.DMA
    orow = rows // 2
    out = pl.pallas_call(
        kernel,
        out_shape=pltpu.VMEM((orow, width), BF16),
        in_specs=[anyspace] * 9,
        out_specs=pl.BlockSpec(memory_space=pltpu.VMEM),
        scratch_shapes=[
            vm((rows, width), BF16),
            vm((rows // CHUNKS, width), BF16),
            vm((rows // CHUNKS, width), BF16),
            vm((rows // CHUNKS, width), BF16),
            vm((1, width), F32),
            pltpu.SMEM(sink_logit.shape, F32),
            vm((qn + 2 * kn, width), BF16),
            vm(wp.shape, BF16),
            vm((width, pn), BF16),
            vm((qn + pn, width), BF16),
            vm((qn, rows), BF16),
            vm((WINDOW + rows, kn), BF16),
            vm((kn, WINDOW + rows), BF16),
            vm((WINDOW + rows, pn), BF16),
            vm((rows, qn + pn), BF16),
            vm((rows, 128), F32),
            vm((8, 128), F32),
            vm((6, WINDOW, 512), F32),
            vm((6, WINDOW, 512), BF16),
            vm((WINDOW, kn), BF16),
            vm((kn, WINDOW), BF16),
            vm((TAIL, 384), BF16),
            vm((WINDOW, kn), BF16),
            vm((kn, WINDOW), BF16),
            vm((TAIL, 384), BF16),
            vm((8, 128), F32),
            vm((GROUP - 1, 8, 128), F32),
            vm((8, 128), F32),
            vm((8, 128), F32),
            vm((orow, width), BF16),
            vm((orow, width), BF16),
            dma((CHUNKS,)),
            dma((8,)),
            dma((CHUNKS,)),
            dma((CHUNKS,)),
            dma((3,)),
            dma((3,)),
            dma((GROUP - 1,)),
            dma((GROUP - 1,)),
            dma((GROUP,)),
            dma(()),
            dma((OUT_CHUNKS,)),
            dma((OUT_CHUNKS,)),
            pltpu.SemaphoreType.REGULAR((GROUP,)),
        ],
        compiler_params=pltpu.CompilerParams(
            collective_id=0, has_side_effects=True, vmem_limit_bytes=60 * 1024 * 1024
        ),
    )(tokens, norm_gain.reshape(1, width), *turned, sink_logit, wp, wa, wpo)
    return out[None]


def solution(mesh):
    in_specs = (
        P("fs", ("grp", "sp"), "tp"),
        P(),
        P(None, "tp", None),
        P(None, "tp", None),
        P(None, "tp", None),
        P("tp"),
        P(None, None, "tp"),
        P("tp", None, None),
        P(None, "tp", None),
    )
    out_specs = P("fs", ("grp", "sp", "tp"), None)
    return jax.shard_map(shards, mesh=mesh, in_specs=in_specs, out_specs=out_specs, check_vma=False)
```

```python
import functools

import jax
import jax.numpy as jnp
from jax import lax
from jax.experimental import pallas as pl
from jax.experimental.pallas import tpu as pltpu
from jax.sharding import PartitionSpec as P

WINDOW = 128
REACHES = (2, 4, 16)
TAIL = 16
GROUP = 4
CHUNKS = 3
OUT_CHUNKS = 2
NEG = -1e30
BF16 = jnp.bfloat16
F32 = jnp.float32
MESH = pl.DeviceIdType.MESH
NT = (((1,), (1,)), ((), ()))


def kernel(
    tok_hbm, gain_hbm, wq_hbm, wk_hbm, wv_hbm, sink_hbm, wp_hbm, wa_hbm, wpo_hbm,
    outbuf,
    tok, nrm0, nrm1, nrm2, gain_ref, sink_ref, wqkv, wpraw, wp, wo, qt, kx, vt, px, att, l3, bt,
    sbuf, pbuf,
    kin, vin, pin, ktail, vtail, ptail, totout, totin, carryout, carryin,
    own0, own1, sendbuf, recvbuf,
    tok_sem, w_sem, tsend, trecv, tail_send, tail_recv, tot_send, tot_recv,
    carry_send, carry_recv, out_send, out_recv, ready,
):
    me = lax.axis_index("tp")
    other = 1 - me
    z = lax.axis_index("sp")
    nz = lax.axis_size("sp")
    rows, width = tok.shape
    nrm = (nrm0, nrm1, nrm2)
    own = (own0, own1)
    half = width // 2
    heads = qt.shape[0] // 64
    kv = kx.shape[1] // 64
    group = heads // kv
    nb = rows // WINDOW
    crow = rows // CHUNKS
    gi = lax.rem(z, GROUP)
    base = z - gi

    def tok_copy(c):
        return pltpu.make_async_copy(
            tok_hbm.at[0, pl.ds(c * crow, crow), :],
            tok.at[pl.ds(c * crow, crow), pl.ds(pl.multiple_of(me * half, half), half)],
            tok_sem.at[c],
        )

    qn, kn = wq_hbm.shape[0], wk_hbm.shape[0]
    loads = [
        pltpu.make_async_copy(wp_hbm, wpraw, w_sem.at[0]),
        pltpu.make_async_copy(wq_hbm, wqkv.at[pl.ds(0, qn)], w_sem.at[1]),
        pltpu.make_async_copy(wk_hbm, wqkv.at[pl.ds(qn, kn)], w_sem.at[2]),
        pltpu.make_async_copy(wv_hbm, wqkv.at[pl.ds(qn + kn, kn)], w_sem.at[3]),
        pltpu.make_async_copy(wa_hbm, wo.at[pl.ds(0, qn)], w_sem.at[4]),
        pltpu.make_async_copy(wpo_hbm, wo.at[pl.ds(qn, wo.shape[0] - qn)], w_sem.at[5]),
        pltpu.make_async_copy(gain_hbm, gain_ref, w_sem.at[6]),
        pltpu.make_async_copy(sink_hbm, sink_ref, w_sem.at[7]),
    ]
    barrier = pltpu.get_barrier_semaphore()
    pl.semaphore_signal(barrier, inc=1, device_id={"tp": other}, device_id_type=MESH)
    for c in reversed(range(CHUNKS)):
        tok_copy(c).start()
    for load in (*loads[6:], *loads[1:4], loads[0], *loads[4:6]):
        load.start()

    def sends_to(d):
        inside = gi + d < GROUP
        leads = gi == GROUP - 1
        return (inside | leads) & (z + d < nz) if d < GROUP else leads & (z + d < nz)

    def hears_from(d):
        return (d <= gi) | ((d == gi + 1) & (base > 0))

    for d in range(1, GROUP + 1):

        @pl.when(sends_to(d))
        def _():
            pl.semaphore_signal(barrier, inc=1, device_id={"sp": z + d}, device_id_type=MESH)

    behind = gi + jnp.where(base > 0, 1, 0)
    pl.semaphore_wait(barrier, 1 + behind)

    def tok_send(c):
        return pltpu.make_async_remote_copy(
            src_ref=tok_hbm.at[0, pl.ds(c * crow, crow), :],
            dst_ref=tok.at[pl.ds(c * crow, crow), pl.ds(pl.multiple_of(me * half, half), half)],
            send_sem=tsend.at[c],
            recv_sem=trecv.at[c],
            device_id={"tp": other},
            device_id_type=MESH,
        )

    for c in reversed(range(CHUNKS)):
        tok_send(c).start()
    for d in range(1, GROUP + 1):

        @pl.when(hears_from(d))
        def _():
            pl.semaphore_signal(ready.at[d - 1], inc=1, device_id={"sp": z - d}, device_id_type=MESH)

    pi = lax.broadcasted_iota(jnp.int32, (256, 256), 0)
    pc = lax.broadcasted_iota(jnp.int32, (256, 256), 1)
    perm = jnp.where(pc == 4 * (pi & 63) + (pi >> 6), 1.0, 0.0).astype(BF16)

    def sort_one(r):
        at = pl.multiple_of(r * 512, 512)
        pair = jnp.concatenate(
            [wpraw[pl.ds(at, 256), :], wpraw[pl.ds(at + 256, 256), :]], axis=1
        )
        got = jnp.dot(perm, pair, preferred_element_type=F32).astype(BF16)
        to = pl.multiple_of(r * 128, 128)
        for g in range(4):
            for s in range(2):
                wp[pl.ds(to + 64 * s, 64), pl.ds(128 * g, 128)] = got[
                    64 * g : 64 * g + 64, 128 * s : 128 * s + 128
                ]

    def norm(c):
        for n in range(crow // 16):
            x = tok[c * crow + 16 * n : c * crow + 16 * (n + 1), :].astype(F32)
            mean = jnp.sum(x * x, axis=1, keepdims=True) * (1.0 / width)
            scale = lax.rsqrt(mean + 1e-06)
            nrm[c][16 * n : 16 * (n + 1), :] = (x * scale * gain).astype(BF16)

    def pool_in(c):
        lo = c * crow
        pooled_in = jnp.dot(nrm[c][...], wp[...], preferred_element_type=F32).astype(BF16)
        px[WINDOW + lo : WINDOW + lo + crow, :] = pooled_in
        for b in range(crow // WINDOW):
            piece = pooled_in[b * WINDOW : (b + 1) * WINDOW, 384:].astype(F32)
            n = c * (crow // WINDOW) + b
            bt[n : n + 1, :] = jnp.sum(piece, axis=0, keepdims=True)

    def qkv_of(c):
        lo = c * crow
        cut = (qn + 2 * kn) // 2
        part = nrm[c][...]
        q = lax.dot_general(wqkv[:cut, :], part, NT, preferred_element_type=F32)
        qkv = lax.dot_general(wqkv[cut:, :], part, NT, preferred_element_type=F32)
        qt[:cut, lo : lo + crow] = (q * 0.125).astype(BF16)
        qt[cut:, lo : lo + crow] = (qkv[: qn - cut] * 0.125).astype(BF16)
        kx[WINDOW + lo : WINDOW + lo + crow, :] = jnp.transpose(
            qkv[qn - cut : qn - cut + kn]
        ).astype(BF16)
        vt[:, WINDOW + lo : WINDOW + lo + crow] = qkv[qn - cut + kn :].astype(BF16)

    def tail_copy(n):
        src, dst = ((ktail, kin), (vtail, vin), (ptail, pin))[n]
        return pltpu.make_async_remote_copy(
            src_ref=src,
            dst_ref=dst,
            send_sem=tail_send.at[n],
            recv_sem=tail_recv.at[n],
            device_id={"sp": z + 1},
            device_id_type=MESH,
        )

    def tot_copy(d):
        return pltpu.make_async_remote_copy(
            src_ref=totout,
            dst_ref=totin.at[d - 1],
            send_sem=tot_send.at[d - 1],
            recv_sem=tot_recv.at[d - 1],
            device_id={"sp": z + d},
            device_id_type=MESH,
        )

    def carry_copy(d):
        return pltpu.make_async_remote_copy(
            src_ref=carryout,
            dst_ref=carryin,
            send_sem=carry_send.at[d - 1],
            recv_sem=carry_recv,
            device_id={"sp": z + d},
            device_id_type=MESH,
        )

    leads = (gi == GROUP - 1) & (z + 1 < nz)

    keyi = lax.broadcasted_iota(jnp.int32, (WINDOW, group * WINDOW), 0)
    posi = lax.broadcasted_iota(jnp.int32, (WINDOW, group * WINDOW), 1) & (WINDOW - 1)
    bi = lax.broadcasted_iota(jnp.int32, (WINDOW, 2 * WINDOW), 0)
    bj = lax.broadcasted_iota(jnp.int32, (WINDOW, 2 * WINDOW), 1)
    gap = bi + WINDOW - bj
    bands = [jnp.where((gap >= 0) & (gap < r), 1.0, 0.0).astype(BF16) for r in REACHES]
    bands.append(jnp.where((gap >= 0) & (bj >= WINDOW), 1.0, 0.0).astype(BF16))

    def counts(b):
        first = z * rows + b * WINDOW + 1
        return (lax.broadcasted_iota(jnp.int32, (WINDOW, 1), 0) + first).astype(F32)

    here = keyi <= posi
    quarter = here[:, :WINDOW]

    def scores(n, b, h):
        lo = b * WINDOW
        qs = jnp.concatenate(
            [
                qt[64 * (group * h + j) : 64 * (group * h + j + 1), lo : lo + WINDOW]
                for j in range(group)
            ],
            axis=1,
        )
        blank = jnp.zeros_like(qs)
        qpad = jnp.concatenate([qs if i == h else blank for i in range(kv)], axis=0)
        s = jnp.dot(kx[lo : lo + 2 * WINDOW, :], qpad, preferred_element_type=F32)
        before = s[:WINDOW]
        if b == 0:
            before = before + jnp.where(z > 0, 0.0, NEG)
        sbuf[n] = jnp.where(here, s[WINDOW:], before)

    def weights(n, b, h):
        for j in range(group):
            s = sbuf[n, :, j * WINDOW : (j + 1) * WINDOW]
            sink = jnp.full((1, WINDOW), sink_ref[group * h + j], F32)
            top = jnp.maximum(jnp.max(s, axis=0, keepdims=True), sink)
            e = jnp.exp(s - top)
            tot = jnp.sum(e, axis=0, keepdims=True) + jnp.exp(sink - top)
            pbuf[n, :, j * WINDOW : (j + 1) * WINDOW] = (e * (1.0 / tot)).astype(BF16)

    def attend(n, b, h):
        lo = b * WINDOW
        w = pbuf[n]
        blank = jnp.zeros_like(w)
        wt = jnp.concatenate([jnp.where(here, blank, w), jnp.where(here, w, blank)], axis=0)
        o = jnp.dot(
            vt[64 * h : 64 * (h + 1), lo : lo + 2 * WINDOW], wt, preferred_element_type=F32
        )
        o = jnp.concatenate([o[:, j * WINDOW : (j + 1) * WINDOW] for j in range(group)], axis=0)
        att[lo : lo + WINDOW, 64 * group * h : 64 * group * (h + 1)] = jnp.transpose(o).astype(BF16)

    def pool(b):
        lo = b * WINDOW
        count = counts(b)
        for g in range(3):
            near = px[lo : lo + 2 * WINDOW, 128 * g : 128 * (g + 1)]
            sums = jnp.dot(bands[g], near, preferred_element_type=F32)
            mean = sums * (1.0 / jnp.minimum(count, float(REACHES[g])))
            att[lo : lo + WINDOW, qn + 128 * g : qn + 128 * (g + 1)] = (
                mean - near[WINDOW:].astype(F32)
            ).astype(BF16)
        near = px[lo : lo + 2 * WINDOW, 384:512]
        l3[lo : lo + WINDOW, :] = jnp.dot(bands[3], near, preferred_element_type=F32)

    def blocks(which, beside=()):
        chains = [(b, h) for b in which for h in range(kv)]
        last = len(chains)
        beside = list(beside)
        for n in range(last + 2):
            if n < last:
                scores(n, *chains[n])
            if 0 <= n - 1 < last:
                weights(n - 1, *chains[n - 1])
            if n % 2 == 1 and beside:
                step, chunk = beside.pop(0)
                step(chunk)
            if 0 <= n - 2 < last:
                attend(n - 2, *chains[n - 2])
                if chains[n - 2][1] == 0:
                    pool(chains[n - 2][0])

    loads[6].wait()
    gain = gain_ref[...]
    tok_copy(2).wait()
    tok_send(2).wait_recv()
    norm(2)
    tok_copy(1).wait()
    tok_send(1).wait_recv()
    for load in loads[1:4]:
        load.wait()

    norm(1)
    qkv_of(2)

    tok_copy(0).wait()
    tok_send(0).wait_recv()
    loads[0].wait()
    norm(0)
    for r in range(width // 128):
        sort_one(r)
    qkv_of(1)
    pool_in(2)

    ktail[...] = kx[rows : rows + WINDOW, :]
    vtail[...] = vt[:, rows : rows + WINDOW]
    ptail[...] = px[WINDOW + rows - TAIL : WINDOW + rows, 0:384]
    px[0:WINDOW, :] = jnp.zeros((WINDOW, px.shape[1]), BF16)
    kx[0:WINDOW, :] = jnp.zeros((WINDOW, kx.shape[1]), BF16)
    vt[:, 0:WINDOW] = jnp.zeros((vt.shape[0], WINDOW), BF16)

    @pl.when(z + 1 < nz)
    def _():
        pl.semaphore_wait(ready.at[0], 1)
        for n in range(3):
            tail_copy(n).start()

    loads[7].wait()

    blocks(range(nb - 1, nb // 2 - 1, -1), ((pool_in, 1), (qkv_of, 0), (pool_in, 0)))

    total = jnp.sum(bt[0:nb, :], axis=0, keepdims=True)
    totout[...] = jnp.broadcast_to(total, totout.shape)
    for d in range(1, GROUP):

        @pl.when(gi + d < GROUP)
        def _():
            if d > 1:
                pl.semaphore_wait(ready.at[d - 1], 1)
            tot_copy(d).start()

    @pl.when(z > 0)
    def _():
        for n in range(3):
            tail_copy(n).wait_recv()
        kx[0:WINDOW, :] = kin[...]
        vt[:, 0:WINDOW] = vin[...]
        px[WINDOW - TAIL : WINDOW, 0:384] = pin[...]

    blocks(range(nb // 2 - 1, -1, -1))

    for d in range(1, GROUP):

        @pl.when(d <= gi)
        def _():
            tot_copy(d).wait_recv()

        @pl.when(d > gi)
        def _():
            totin[d - 1] = jnp.zeros(totin.shape[1:], F32)

    @pl.when(base > 0)
    def _():
        carry_copy(1).wait_recv()

    @pl.when(base == 0)
    def _():
        carryin[...] = jnp.zeros(carryin.shape, F32)

    carried = carryin[...]
    for d in range(1, GROUP):
        carried = carried + totin[d - 1]

    @pl.when(leads)
    def _():
        carryout[...] = carried + totout[...]
        for d in range(1, GROUP + 1):
            if d > 1:
                pl.semaphore_wait(ready.at[d - 1], 1)
            carry_copy(d).start()

    run = carried[0:1, :]
    for b in range(nb):
        lo = b * WINDOW
        mean = (l3[lo : lo + WINDOW, :] + run) * (1.0 / counts(b))
        run = run + bt[b : b + 1, :]
        att[lo : lo + WINDOW, qn + 384 :] = (
            mean - px[WINDOW + lo : WINDOW + lo + WINDOW, 384:].astype(F32)
        ).astype(BF16)

    orow = rows // 2
    ocol = width // OUT_CHUNKS
    for load in loads[4:6]:
        load.wait()

    def out_copy(n):
        cols = pl.ds(n * ocol, ocol)
        return pltpu.make_async_remote_copy(
            src_ref=sendbuf.at[:, cols],
            dst_ref=recvbuf.at[:, cols],
            send_sem=out_send.at[n],
            recv_sem=out_recv.at[n],
            device_id={"tp": other},
            device_id_type=MESH,
        )

    theirs = pl.ds(pl.multiple_of(other * orow, orow), orow)
    ours = pl.ds(pl.multiple_of(me * orow, orow), orow)
    for n in range(OUT_CHUNKS):
        cols = slice(n * ocol, (n + 1) * ocol)
        sendbuf[:, cols] = jnp.dot(
            att[theirs, :], wo[:, cols], preferred_element_type=F32
        ).astype(BF16)
        out_copy(n).start()
    def add(n):
        cols = slice(n * ocol, (n + 1) * ocol)
        outbuf[:, cols] = (own[n][...] + recvbuf[:, cols].astype(F32)).astype(BF16)

    for n in range(OUT_CHUNKS):
        cols = slice(n * ocol, (n + 1) * ocol)
        own[n][...] = jnp.dot(att[ours, :], wo[:, cols], preferred_element_type=F32)
    for n in range(OUT_CHUNKS):
        out_copy(n).wait_recv()
        add(n)

    for c in range(CHUNKS):
        tok_send(c).wait_send()
    for d in range(1, GROUP):

        @pl.when(gi + d < GROUP)
        def _():
            tot_copy(d).wait_send()

    @pl.when(z + 1 < nz)
    def _():
        for n in range(3):
            tail_copy(n).wait_send()

    @pl.when(leads)
    def _():
        for d in range(1, GROUP + 1):
            carry_copy(d).wait_send()

    for n in range(OUT_CHUNKS):
        out_copy(n).wait_send()


def shards(
    tokens,
    norm_gain,
    query_weight,
    key_weight,
    value_weight,
    sink_logit,
    pool_weight,
    attn_out_weight,
    pool_out_weight,
):
    rows, half = tokens.shape[1:]
    width = 2 * half
    assert lax.axis_size("tp") == 2 and lax.axis_size("sp") % GROUP == 0
    turned = [
        jnp.transpose(w, (1, 2, 0)).reshape(-1, width)
        for w in (query_weight, key_weight, value_weight)
    ]
    qn, kn = turned[0].shape[0], turned[1].shape[0]
    pn = pool_weight.shape[1] * pool_weight.shape[2]
    wp = pool_weight.reshape(-1, pool_weight.shape[2])
    wa = attn_out_weight.reshape(-1, width)
    wpo = pool_out_weight.reshape(-1, width)
    anyspace = pl.BlockSpec(memory_space=pl.ANY)
    vm = pltpu.VMEM
    dma = pltpu.SemaphoreType.DMA
    orow = rows // 2
    out = pl.pallas_call(
        kernel,
        out_shape=pltpu.VMEM((orow, width), BF16),
        in_specs=[anyspace] * 9,
        out_specs=pl.BlockSpec(memory_space=pltpu.VMEM),
        scratch_shapes=[
            vm((rows, width), BF16),
            vm((rows // CHUNKS, width), BF16),
            vm((rows // CHUNKS, width), BF16),
            vm((rows // CHUNKS, width), BF16),
            vm((1, width), F32),
            pltpu.SMEM(sink_logit.shape, F32),
            vm((qn + 2 * kn, width), BF16),
            vm(wp.shape, BF16),
            vm((width, pn), BF16),
            vm((qn + pn, width), BF16),
            vm((qn, rows), BF16),
            vm((WINDOW + rows, kn), BF16),
            vm((kn, WINDOW + rows), BF16),
            vm((WINDOW + rows, pn), BF16),
            vm((rows, qn + pn), BF16),
            vm((rows, 128), F32),
            vm((8, 128), F32),
            vm((6, WINDOW, 512), F32),
            vm((6, WINDOW, 512), BF16),
            vm((WINDOW, kn), BF16),
            vm((kn, WINDOW), BF16),
            vm((TAIL, 384), BF16),
            vm((WINDOW, kn), BF16),
            vm((kn, WINDOW), BF16),
            vm((TAIL, 384), BF16),
            vm((8, 128), F32),
            vm((GROUP - 1, 8, 128), F32),
            vm((8, 128), F32),
            vm((8, 128), F32),
            vm((orow, width // OUT_CHUNKS), F32),
            vm((orow, width // OUT_CHUNKS), F32),
            vm((orow, width), BF16),
            vm((orow, width), BF16),
            dma((CHUNKS,)),
            dma((8,)),
            dma((CHUNKS,)),
            dma((CHUNKS,)),
            dma((3,)),
            dma((3,)),
            dma((GROUP - 1,)),
            dma((GROUP - 1,)),
            dma((GROUP,)),
            dma(()),
            dma((OUT_CHUNKS,)),
            dma((OUT_CHUNKS,)),
            pltpu.SemaphoreType.REGULAR((GROUP,)),
        ],
        compiler_params=pltpu.CompilerParams(
            collective_id=0, has_side_effects=True, vmem_limit_bytes=60 * 1024 * 1024
        ),
    )(tokens, norm_gain.reshape(1, width), *turned, sink_logit, wp, wa, wpo)
    return out[None]


def solution(mesh):
    in_specs = (
        P("fs", ("grp", "sp"), "tp"),
        P(),
        P(None, "tp", None),
        P(None, "tp", None),
        P(None, "tp", None),
        P("tp"),
        P(None, None, "tp"),
        P("tp", None, None),
        P(None, "tp", None),
    )
    out_specs = P("fs", ("grp", "sp", "tp"), None)
    return jax.shard_map(shards, mesh=mesh, in_specs=in_specs, out_specs=out_specs, check_vma=False)
```

```python
import functools

import jax
import jax.numpy as jnp
from jax import lax
from jax.experimental import pallas as pl
from jax.experimental.pallas import tpu as pltpu
from jax.sharding import PartitionSpec as P

WINDOW = 128
REACHES = (2, 4, 16)
TAIL = 16
GROUP = 4
CHUNKS = 3
PARTS = ((4, 1), (5, 1), (2, 2), (0, 2))
OUT_CHUNKS = 2
NEG = -1e30
BF16 = jnp.bfloat16
F32 = jnp.float32
MESH = pl.DeviceIdType.MESH
NT = (((1,), (1,)), ((), ()))


def kernel(
    tok_hbm, gain_hbm, wq_hbm, wk_hbm, wv_hbm, sink_hbm, wp_hbm, wa_hbm, wpo_hbm,
    outbuf,
    tok, nrm0, nrm1, nrm2, gain_ref, sink_ref, wqkv, wpraw, wp, wo, qt, kx, vt, px, att, l3, bt,
    sbuf, pbuf, masks,
    kin, vin, pin, ktail, vtail, ptail, totout, totin, carryout, carryin,
    own0, own1, sendbuf, recvbuf,
    tok_sem, w_sem, tsend, trecv, tail_send, tail_recv, tot_send, tot_recv,
    carry_send, carry_recv, out_send, out_recv, ready,
):
    me = lax.axis_index("tp")
    other = 1 - me
    z = lax.axis_index("sp")
    nz = lax.axis_size("sp")
    rows, width = tok.shape
    nrm = (nrm0, nrm1, nrm2)
    own = (own0, own1)
    half = width // 2
    heads = qt.shape[0] // 64
    kv = kx.shape[1] // 64
    group = heads // kv
    nb = rows // WINDOW
    crow = rows // CHUNKS
    gi = lax.rem(z, GROUP)
    base = z - gi

    mine = pl.ds(pl.multiple_of(me * half, half), half)

    def tok_copy(c):
        return pltpu.make_async_copy(
            tok_hbm.at[0, pl.ds(c * crow, crow), :],
            tok.at[pl.ds(c * crow, crow), mine],
            tok_sem.at[c],
        )

    qn, kn = wq_hbm.shape[0], wk_hbm.shape[0]
    loads = [
        pltpu.make_async_copy(wp_hbm, wpraw, w_sem.at[0]),
        pltpu.make_async_copy(wq_hbm, wqkv.at[pl.ds(0, qn)], w_sem.at[1]),
        pltpu.make_async_copy(wk_hbm, wqkv.at[pl.ds(qn, kn)], w_sem.at[2]),
        pltpu.make_async_copy(wv_hbm, wqkv.at[pl.ds(qn + kn, kn)], w_sem.at[3]),
        pltpu.make_async_copy(wa_hbm, wo.at[pl.ds(0, qn)], w_sem.at[4]),
        pltpu.make_async_copy(wpo_hbm, wo.at[pl.ds(qn, wo.shape[0] - qn)], w_sem.at[5]),
        pltpu.make_async_copy(gain_hbm, gain_ref, w_sem.at[6]),
        pltpu.make_async_copy(sink_hbm, sink_ref, w_sem.at[7]),
    ]
    barrier = pltpu.get_barrier_semaphore()
    pl.semaphore_signal(barrier, inc=1, device_id={"tp": other}, device_id_type=MESH)
    tok_copy(2).start()
    for load in (*loads[6:], *loads[1:4]):
        load.start()

    @pl.when(me == 1)
    def _():
        tok_copy(1).start()
        tok_copy(0).start()


    def sends_to(d):
        inside = gi + d < GROUP
        leads = gi == GROUP - 1
        return (inside | leads) & (z + d < nz) if d < GROUP else leads & (z + d < nz)

    def hears_from(d):
        return (d <= gi) | ((d == gi + 1) & (base > 0))

    for d in range(1, GROUP + 1):

        @pl.when(sends_to(d))
        def _():
            pl.semaphore_signal(barrier, inc=1, device_id={"sp": z + d}, device_id_type=MESH)

    behind = gi + jnp.where(base > 0, 1, 0)
    pl.semaphore_wait(barrier, 1 + behind)

    def tok_send(n, loaded=False):
        first, count = PARTS[n]
        spot = pl.ds(first * WINDOW, count * WINDOW)
        return pltpu.make_async_remote_copy(
            src_ref=tok.at[spot, mine] if loaded else tok_hbm.at[0, spot, :],
            dst_ref=tok.at[spot, mine],
            send_sem=tsend.at[n],
            recv_sem=trecv.at[n],
            device_id={"tp": other},
            device_id_type=MESH,
        )

    @pl.when(me == 0)
    def _():
        for n in range(len(PARTS)):
            tok_send(n).start()

    @pl.when(me == 1)
    def _():
        for c in reversed(range(CHUNKS)):
            tok_copy(c).wait()
        for n in range(len(PARTS)):
            tok_send(n, True).start()

    for d in range(1, GROUP + 1):

        @pl.when(hears_from(d))
        def _():
            pl.semaphore_signal(ready.at[d - 1], inc=1, device_id={"sp": z - d}, device_id_type=MESH)

    pi = lax.broadcasted_iota(jnp.int32, (256, 256), 0)
    pc = lax.broadcasted_iota(jnp.int32, (256, 256), 1)
    perm = jnp.where(pc == 4 * (pi & 63) + (pi >> 6), 1.0, 0.0).astype(BF16)

    def sort_one(r):
        at = pl.multiple_of(r * 512, 512)
        pair = jnp.concatenate(
            [wpraw[pl.ds(at, 256), :], wpraw[pl.ds(at + 256, 256), :]], axis=1
        )
        got = jnp.dot(perm, pair, preferred_element_type=F32).astype(BF16)
        to = pl.multiple_of(r * 128, 128)
        for g in range(4):
            for s in range(2):
                wp[pl.ds(to + 64 * s, 64), pl.ds(128 * g, 128)] = got[
                    64 * g : 64 * g + 64, 128 * s : 128 * s + 128
                ]

    def norm(c, low=0, high=crow // 16):
        for n in range(low, high):
            x = tok[c * crow + 16 * n : c * crow + 16 * (n + 1), :].astype(F32)
            mean = jnp.sum(x * x, axis=1, keepdims=True) * (1.0 / width)
            scale = lax.rsqrt(mean + 1e-06)
            nrm[c][16 * n : 16 * (n + 1), :] = (x * scale * gain).astype(BF16)

    def pool_in(c, part=None):
        lo = c * crow
        for p in (0, 1) if part is None else (part,):
            cols = slice(256 * p, 256 * (p + 1))
            pooled_in = jnp.dot(nrm[c][...], wp[:, cols], preferred_element_type=F32).astype(BF16)
            px[WINDOW + lo : WINDOW + lo + crow, cols] = pooled_in
            if p == 1:
                for b in range(crow // WINDOW):
                    piece = pooled_in[b * WINDOW : (b + 1) * WINDOW, 128:].astype(F32)
                    n = c * (crow // WINDOW) + b
                    bt[n : n + 1, :] = jnp.sum(piece, axis=0, keepdims=True)

    def qkv_of(c):
        lo = c * crow
        cut = (qn + 2 * kn) // 2
        part = nrm[c][...]
        q = lax.dot_general(wqkv[:cut, :], part, NT, preferred_element_type=F32)
        qkv = lax.dot_general(wqkv[cut:, :], part, NT, preferred_element_type=F32)
        qt[:cut, lo : lo + crow] = (q * 0.125).astype(BF16)
        qt[cut:, lo : lo + crow] = (qkv[: qn - cut] * 0.125).astype(BF16)
        kx[WINDOW + lo : WINDOW + lo + crow, :] = jnp.transpose(
            qkv[qn - cut : qn - cut + kn]
        ).astype(BF16)
        vt[:, WINDOW + lo : WINDOW + lo + crow] = qkv[qn - cut + kn :].astype(BF16)

    def tail_copy(n):
        src, dst = ((ktail, kin), (vtail, vin), (ptail, pin))[n]
        return pltpu.make_async_remote_copy(
            src_ref=src,
            dst_ref=dst,
            send_sem=tail_send.at[n],
            recv_sem=tail_recv.at[n],
            device_id={"sp": z + 1},
            device_id_type=MESH,
        )

    def tot_copy(d):
        return pltpu.make_async_remote_copy(
            src_ref=totout,
            dst_ref=totin.at[d - 1],
            send_sem=tot_send.at[d - 1],
            recv_sem=tot_recv.at[d - 1],
            device_id={"sp": z + d},
            device_id_type=MESH,
        )

    def carry_copy(d):
        return pltpu.make_async_remote_copy(
            src_ref=carryout,
            dst_ref=carryin,
            send_sem=carry_send.at[d - 1],
            recv_sem=carry_recv,
            device_id={"sp": z + d},
            device_id_type=MESH,
        )

    leads = (gi == GROUP - 1) & (z + 1 < nz)

    keyi = lax.broadcasted_iota(jnp.int32, (WINDOW, group * WINDOW), 0)
    posi = lax.broadcasted_iota(jnp.int32, (WINDOW, group * WINDOW), 1) & (WINDOW - 1)
    bi = lax.broadcasted_iota(jnp.int32, (WINDOW, 2 * WINDOW), 0)
    bj = lax.broadcasted_iota(jnp.int32, (WINDOW, 2 * WINDOW), 1)
    gap = bi + WINDOW - bj
    bands = [jnp.where((gap >= 0) & (gap < r), 1.0, 0.0).astype(BF16) for r in REACHES]
    bands.append(jnp.where((gap >= 0) & (bj >= WINDOW), 1.0, 0.0).astype(BF16))

    def counts(b):
        first = z * rows + b * WINDOW + 1
        return (lax.broadcasted_iota(jnp.int32, (WINDOW, 1), 0) + first).astype(F32)

    here = keyi <= posi
    masks[1] = jnp.where(here, 1.0, 0.0).astype(BF16)
    masks[0] = jnp.where(here, 0.0, 1.0).astype(BF16)

    def scores(n, b, h):
        lo = b * WINDOW
        qs = jnp.concatenate(
            [
                qt[64 * (group * h + j) : 64 * (group * h + j + 1), lo : lo + WINDOW]
                for j in range(group)
            ],
            axis=1,
        )
        blank = jnp.zeros_like(qs)
        qpad = jnp.concatenate([qs if i == h else blank for i in range(kv)], axis=0)
        s = jnp.dot(kx[lo : lo + 2 * WINDOW, :], qpad, preferred_element_type=F32)
        before = s[:WINDOW]
        if b == 0:
            before = before + jnp.where(z > 0, 0.0, NEG)
        sbuf[n] = jnp.where(here, s[WINDOW:], before)

    def weights(n, b, h):
        for j in range(0, group, 2):
            s = sbuf[n, :, j * WINDOW : (j + 2) * WINDOW]
            sink = jnp.concatenate(
                [jnp.full((1, WINDOW), sink_ref[group * h + j + i], F32) for i in range(2)], axis=1
            )
            top = jnp.maximum(jnp.max(s, axis=0, keepdims=True), sink)
            e = jnp.exp(s - top)
            tot = jnp.sum(e, axis=0, keepdims=True) + jnp.exp(sink - top)
            pbuf[n, :, j * WINDOW : (j + 2) * WINDOW] = (e * (1.0 / tot)).astype(BF16)

    def attend(n, b, h):
        lo = b * WINDOW
        w = pbuf[n]
        wt = jnp.concatenate([w * masks[0], w * masks[1]], axis=0)
        o = jnp.dot(
            vt[64 * h : 64 * (h + 1), lo : lo + 2 * WINDOW], wt, preferred_element_type=F32
        )
        o = jnp.concatenate([o[:, j * WINDOW : (j + 1) * WINDOW] for j in range(group)], axis=0)
        att[lo : lo + WINDOW, 64 * group * h : 64 * group * (h + 1)] = jnp.transpose(o).astype(BF16)

    def pool(b):
        spots = [n * WINDOW for n in (b, b + 1)]

        def both(g):
            return jnp.concatenate(
                [px[lo : lo + 2 * WINDOW, 128 * g : 128 * (g + 1)] for lo in spots], axis=1
            )

        means = []
        for g in range(3):
            near = both(g)
            sums = jnp.dot(bands[g], near, preferred_element_type=F32)
            here_in = near[WINDOW:].astype(F32)
            for n in range(2):
                part = slice(n * WINDOW, (n + 1) * WINDOW)
                scale = 1.0 / jnp.minimum(counts(b + n), float(REACHES[g]))
                means.append((sums[:, part] * scale - here_in[:, part]).astype(BF16))
        for n, lo in enumerate(spots):
            att[lo : lo + WINDOW, qn : qn + 256] = jnp.concatenate([means[n], means[2 + n]], axis=1)
            att[lo : lo + WINDOW, qn + 256 : qn + 384] = means[4 + n]
        sums = jnp.dot(bands[3], both(3), preferred_element_type=F32)
        for n, lo in enumerate(spots):
            l3[lo : lo + WINDOW, :] = sums[:, n * WINDOW : (n + 1) * WINDOW]

    def blocks(which, spots, beside):
        chains = [(b, h) for b in which for h in range(kv)]
        last = len(chains)
        beside = list(beside)
        for n in range(last + 6):
            if n < last:
                scores(n, *chains[n])
            if 0 <= n - 3 < last:
                weights(n - 3, *chains[n - 3])
            while spots and spots[0] == n:
                spots = spots[1:]
                step, *what = beside.pop(0)
                step(*what)
            if 0 <= n - 6 < last:
                attend(n - 6, *chains[n - 6])

    loads[6].wait()
    gain = gain_ref[...]

    @pl.when(me == 0)
    def _():
        tok_copy(2).wait()
        tok_copy(1).start()
        tok_copy(0).start()

    loads[0].start()
    tok_send(0).wait_recv()
    norm(2, 0, crow // 32)
    tok_send(1).wait_recv()
    norm(2, crow // 32)
    for load in loads[1:4]:
        load.wait()

    qkv_of(2)

    loads[4].start()
    loads[5].start()

    @pl.when(me == 0)
    def _():
        tok_copy(1).wait()
        tok_copy(0).wait()

    tok_send(2).wait_recv()
    tok_send(3).wait_recv()
    loads[0].wait()
    for r in range(width // 128):
        sort_one(r)
    norm(1)
    pool_in(2)
    norm(0)
    qkv_of(1)

    ktail[...] = kx[rows : rows + WINDOW, :]
    vtail[...] = vt[:, rows : rows + WINDOW]
    ptail[...] = px[WINDOW + rows - TAIL : WINDOW + rows, 0:384]
    px[0:WINDOW, :] = jnp.zeros((WINDOW, px.shape[1]), BF16)
    kx[0:WINDOW, :] = jnp.zeros((WINDOW, kx.shape[1]), BF16)
    vt[:, 0:WINDOW] = jnp.zeros((vt.shape[0], WINDOW), BF16)

    @pl.when(z + 1 < nz)
    def _():
        pl.semaphore_wait(ready.at[0], 1)
        for n in range(3):
            tail_copy(n).start()

    loads[7].wait()

    blocks(range(nb - 1, nb // 2 - 1, -1), (1, 3, 5), ((pool_in, 1, 1), (qkv_of, 0), (pool_in, 0, 1)))

    total = jnp.sum(bt[0:nb, :], axis=0, keepdims=True)
    totout[...] = jnp.broadcast_to(total, totout.shape)
    for d in range(1, GROUP):

        @pl.when(gi + d < GROUP)
        def _():
            if d > 1:
                pl.semaphore_wait(ready.at[d - 1], 1)
            tot_copy(d).start()

    @pl.when(z > 0)
    def _():
        for n in range(3):
            tail_copy(n).wait_recv()
        kx[0:WINDOW, :] = kin[...]
        vt[:, 0:WINDOW] = vin[...]
        px[WINDOW - TAIL : WINDOW, 0:384] = pin[...]

    blocks(range(nb // 2 - 1, -1, -1), (5, 5, 9, 10, 11), ((pool_in, 1, 0), (pool_in, 0, 0), (pool, 4), (pool, 2), (pool, 0)))

    for d in range(1, GROUP):

        @pl.when(d <= gi)
        def _():
            tot_copy(d).wait_recv()

        @pl.when(d > gi)
        def _():
            totin[d - 1] = jnp.zeros(totin.shape[1:], F32)

    @pl.when(base > 0)
    def _():
        carry_copy(1).wait_recv()

    @pl.when(base == 0)
    def _():
        carryin[...] = jnp.zeros(carryin.shape, F32)

    carried = carryin[...]
    for d in range(1, GROUP):
        carried = carried + totin[d - 1]

    @pl.when(leads)
    def _():
        carryout[...] = carried + totout[...]
        for d in range(1, GROUP + 1):
            if d > 1:
                pl.semaphore_wait(ready.at[d - 1], 1)
            carry_copy(d).start()

    run = carried[0:1, :]
    for b in range(nb):
        lo = b * WINDOW
        mean = (l3[lo : lo + WINDOW, :] + run) * (1.0 / counts(b))
        run = run + bt[b : b + 1, :]
        att[lo : lo + WINDOW, qn + 384 :] = (
            mean - px[WINDOW + lo : WINDOW + lo + WINDOW, 384:].astype(F32)
        ).astype(BF16)

    orow = rows // 2
    ocol = width // OUT_CHUNKS
    for load in loads[4:6]:
        load.wait()

    def out_copy(n):
        cols = pl.ds(n * ocol, ocol)
        return pltpu.make_async_remote_copy(
            src_ref=sendbuf.at[:, cols],
            dst_ref=recvbuf.at[:, cols],
            send_sem=out_send.at[n],
            recv_sem=out_recv.at[n],
            device_id={"tp": other},
            device_id_type=MESH,
        )

    theirs = pl.ds(pl.multiple_of(other * orow, orow), orow)
    ours = pl.ds(pl.multiple_of(me * orow, orow), orow)
    for n in range(OUT_CHUNKS):
        cols = slice(n * ocol, (n + 1) * ocol)
        sendbuf[:, cols] = jnp.dot(
            att[theirs, :], wo[:, cols], preferred_element_type=F32
        ).astype(BF16)
        out_copy(n).start()
    def add(n):
        cols = slice(n * ocol, (n + 1) * ocol)
        outbuf[:, cols] = (own[n][...] + recvbuf[:, cols].astype(F32)).astype(BF16)

    for n in range(OUT_CHUNKS):
        cols = slice(n * ocol, (n + 1) * ocol)
        own[n][...] = jnp.dot(att[ours, :], wo[:, cols], preferred_element_type=F32)
    for n in range(OUT_CHUNKS):
        out_copy(n).wait_recv()
        add(n)

    for n in range(len(PARTS)):
        tok_send(n).wait_send()
    for d in range(1, GROUP):

        @pl.when(gi + d < GROUP)
        def _():
            tot_copy(d).wait_send()

    @pl.when(z + 1 < nz)
    def _():
        for n in range(3):
            tail_copy(n).wait_send()

    @pl.when(leads)
    def _():
        for d in range(1, GROUP + 1):
            carry_copy(d).wait_send()

    for n in range(OUT_CHUNKS):
        out_copy(n).wait_send()


def shards(
    tokens,
    norm_gain,
    query_weight,
    key_weight,
    value_weight,
    sink_logit,
    pool_weight,
    attn_out_weight,
    pool_out_weight,
):
    rows, half = tokens.shape[1:]
    width = 2 * half
    assert lax.axis_size("tp") == 2 and lax.axis_size("sp") % GROUP == 0
    turned = [
        jnp.transpose(w, (1, 2, 0)).reshape(-1, width)
        for w in (query_weight, key_weight, value_weight)
    ]
    qn, kn = turned[0].shape[0], turned[1].shape[0]
    pn = pool_weight.shape[1] * pool_weight.shape[2]
    wp = pool_weight.reshape(-1, pool_weight.shape[2])
    wa = attn_out_weight.reshape(-1, width)
    wpo = pool_out_weight.reshape(-1, width)
    anyspace = pl.BlockSpec(memory_space=pl.ANY)
    vm = pltpu.VMEM
    dma = pltpu.SemaphoreType.DMA
    orow = rows // 2
    out = pl.pallas_call(
        kernel,
        out_shape=pltpu.VMEM((orow, width), BF16),
        in_specs=[anyspace] * 9,
        out_specs=pl.BlockSpec(memory_space=pltpu.VMEM),
        scratch_shapes=[
            vm((rows, width), BF16),
            vm((rows // CHUNKS, width), BF16),
            vm((rows // CHUNKS, width), BF16),
            vm((rows // CHUNKS, width), BF16),
            vm((1, width), F32),
            pltpu.SMEM(sink_logit.shape, F32),
            vm((qn + 2 * kn, width), BF16),
            vm(wp.shape, BF16),
            vm((width, pn), BF16),
            vm((qn + pn, width), BF16),
            vm((qn, rows), BF16),
            vm((WINDOW + rows, kn), BF16),
            vm((kn, WINDOW + rows), BF16),
            vm((WINDOW + rows, pn), BF16),
            vm((rows, qn + pn), BF16),
            vm((rows, 128), F32),
            vm((8, 128), F32),
            vm((6, WINDOW, 512), F32),
            vm((6, WINDOW, 512), BF16),
            vm((2, WINDOW, 512), BF16),
            vm((WINDOW, kn), BF16),
            vm((kn, WINDOW), BF16),
            vm((TAIL, 384), BF16),
            vm((WINDOW, kn), BF16),
            vm((kn, WINDOW), BF16),
            vm((TAIL, 384), BF16),
            vm((8, 128), F32),
            vm((GROUP - 1, 8, 128), F32),
            vm((8, 128), F32),
            vm((8, 128), F32),
            vm((orow, width // OUT_CHUNKS), F32),
            vm((orow, width // OUT_CHUNKS), F32),
            vm((orow, width), BF16),
            vm((orow, width), BF16),
            dma((CHUNKS,)),
            dma((8,)),
            dma((len(PARTS),)),
            dma((len(PARTS),)),
            dma((3,)),
            dma((3,)),
            dma((GROUP - 1,)),
            dma((GROUP - 1,)),
            dma((GROUP,)),
            dma(()),
            dma((OUT_CHUNKS,)),
            dma((OUT_CHUNKS,)),
            pltpu.SemaphoreType.REGULAR((GROUP,)),
        ],
        compiler_params=pltpu.CompilerParams(
            collective_id=0, has_side_effects=True, vmem_limit_bytes=60 * 1024 * 1024
        ),
    )(tokens, norm_gain.reshape(1, width), *turned, sink_logit, wp, wa, wpo)
    return out[None]


def solution(mesh):
    in_specs = (
        P("fs", ("grp", "sp"), "tp"),
        P(),
        P(None, "tp", None),
        P(None, "tp", None),
        P(None, "tp", None),
        P("tp"),
        P(None, None, "tp"),
        P("tp", None, None),
        P(None, "tp", None),
    )
    out_specs = P("fs", ("grp", "sp", "tp"), None)
    return jax.shard_map(shards, mesh=mesh, in_specs=in_specs, out_specs=out_specs, check_vma=False)
```

```python
import functools

import jax
import jax.numpy as jnp
from jax import lax
from jax.experimental import pallas as pl
from jax.experimental.pallas import tpu as pltpu
from jax.sharding import PartitionSpec as P

WINDOW = 128
REACHES = (2, 4, 16)
TAIL = 16
GROUP = 4
CHUNKS = 3
PARTS = ((4, 1), (5, 1), (2, 2), (0, 2))
OUT_CHUNKS = 2
NEG = -1e30
BF16 = jnp.bfloat16
F32 = jnp.float32
MESH = pl.DeviceIdType.MESH
NT = (((1,), (1,)), ((), ()))


def kernel(
    tok_hbm, gain_hbm, wq_hbm, wk_hbm, wv_hbm, sink_hbm, wp_hbm, wa_hbm, wpo_hbm,
    outbuf,
    tok, nrm0, nrm1, nrm2, gain_ref, sink_ref, wqkv, wpraw, wp, wo, qt, kx, vt, px, att, l3, bt,
    sbuf, pbuf, masks,
    kin, vin, pin, ktail, vtail, ptail, totout, totin, carryout, carryin,
    own0, own1, sendbuf, recvbuf,
    tok_sem, w_sem, tsend, trecv, tail_send, tail_recv, tot_send, tot_recv,
    carry_send, carry_recv, out_send, out_recv, ready,
):
    me = lax.axis_index("tp")
    other = 1 - me
    z = lax.axis_index("sp")
    nz = lax.axis_size("sp")
    rows, width = tok.shape
    nrm = (nrm0, nrm1, nrm2)
    own = (own0, own1)
    half = width // 2
    heads = qt.shape[0] // 64
    kv = kx.shape[1] // 64
    group = heads // kv
    nb = rows // WINDOW
    crow = rows // CHUNKS
    gi = lax.rem(z, GROUP)
    base = z - gi

    mine = pl.ds(pl.multiple_of(me * half, half), half)

    def tok_copy(c):
        return pltpu.make_async_copy(
            tok_hbm.at[0, pl.ds(c * crow, crow), :],
            tok.at[pl.ds(c * crow, crow), mine],
            tok_sem.at[c],
        )

    qn, kn = wq_hbm.shape[0], wk_hbm.shape[0]
    loads = [
        pltpu.make_async_copy(wp_hbm, wpraw, w_sem.at[0]),
        pltpu.make_async_copy(wq_hbm, wqkv.at[pl.ds(0, qn)], w_sem.at[1]),
        pltpu.make_async_copy(wk_hbm, wqkv.at[pl.ds(qn, kn)], w_sem.at[2]),
        pltpu.make_async_copy(wv_hbm, wqkv.at[pl.ds(qn + kn, kn)], w_sem.at[3]),
        pltpu.make_async_copy(wa_hbm, wo.at[pl.ds(0, qn)], w_sem.at[4]),
        pltpu.make_async_copy(wpo_hbm, wo.at[pl.ds(qn, wo.shape[0] - qn)], w_sem.at[5]),
        pltpu.make_async_copy(gain_hbm, gain_ref, w_sem.at[6]),
        pltpu.make_async_copy(sink_hbm, sink_ref, w_sem.at[7]),
    ]
    barrier = pltpu.get_barrier_semaphore()
    pl.semaphore_signal(barrier, inc=1, device_id={"tp": other}, device_id_type=MESH)
    tok_copy(2).start()
    for load in (*loads[6:], loads[0]):
        load.start()

    @pl.when(me == 1)
    def _():
        tok_copy(1).start()
        tok_copy(0).start()


    def sends_to(d):
        inside = gi + d < GROUP
        leads = gi == GROUP - 1
        return (inside | leads) & (z + d < nz) if d < GROUP else leads & (z + d < nz)

    def hears_from(d):
        return (d <= gi) | ((d == gi + 1) & (base > 0))

    for d in range(1, GROUP + 1):

        @pl.when(sends_to(d))
        def _():
            pl.semaphore_signal(barrier, inc=1, device_id={"sp": z + d}, device_id_type=MESH)

    behind = gi + jnp.where(base > 0, 1, 0)
    pl.semaphore_wait(barrier, 1 + behind)

    def tok_send(n, loaded=False):
        first, count = PARTS[n]
        spot = pl.ds(first * WINDOW, count * WINDOW)
        return pltpu.make_async_remote_copy(
            src_ref=tok.at[spot, mine] if loaded else tok_hbm.at[0, spot, :],
            dst_ref=tok.at[spot, mine],
            send_sem=tsend.at[n],
            recv_sem=trecv.at[n],
            device_id={"tp": other},
            device_id_type=MESH,
        )

    @pl.when(me == 0)
    def _():
        for n in range(len(PARTS)):
            tok_send(n).start()

    @pl.when(me == 1)
    def _():
        for c in reversed(range(CHUNKS)):
            tok_copy(c).wait()
        for n in range(len(PARTS)):
            tok_send(n, True).start()

    for d in range(1, GROUP + 1):

        @pl.when(hears_from(d))
        def _():
            pl.semaphore_signal(ready.at[d - 1], inc=1, device_id={"sp": z - d}, device_id_type=MESH)

    pi = lax.broadcasted_iota(jnp.int32, (256, 256), 0)
    pc = lax.broadcasted_iota(jnp.int32, (256, 256), 1)
    perm = jnp.where(pc == 4 * (pi & 63) + (pi >> 6), 1.0, 0.0).astype(BF16)

    def sort_one(r):
        at = pl.multiple_of(r * 512, 512)
        pair = jnp.concatenate(
            [wpraw[pl.ds(at, 256), :], wpraw[pl.ds(at + 256, 256), :]], axis=1
        )
        got = jnp.dot(perm, pair, preferred_element_type=F32).astype(BF16)
        to = pl.multiple_of(r * 128, 128)
        for g in range(4):
            for s in range(2):
                wp[pl.ds(to + 64 * s, 64), pl.ds(128 * g, 128)] = got[
                    64 * g : 64 * g + 64, 128 * s : 128 * s + 128
                ]

    def norm(c, low=0, high=crow // 16):
        for n in range(low, high):
            x = tok[c * crow + 16 * n : c * crow + 16 * (n + 1), :].astype(F32)
            mean = jnp.sum(x * x, axis=1, keepdims=True) * (1.0 / width)
            scale = lax.rsqrt(mean + 1e-06)
            nrm[c][16 * n : 16 * (n + 1), :] = (x * scale * gain).astype(BF16)

    def pool_in(c, part=None):
        lo = c * crow
        for p in (0, 1) if part is None else (part,):
            cols = slice(256 * p, 256 * (p + 1))
            pooled_in = jnp.dot(nrm[c][...], wp[:, cols], preferred_element_type=F32).astype(BF16)
            px[WINDOW + lo : WINDOW + lo + crow, cols] = pooled_in
            if p == 1:
                for b in range(crow // WINDOW):
                    piece = pooled_in[b * WINDOW : (b + 1) * WINDOW, 128:].astype(F32)
                    n = c * (crow // WINDOW) + b
                    bt[n : n + 1, :] = jnp.sum(piece, axis=0, keepdims=True)

    def qkv_of(c):
        lo = c * crow
        cut = (qn + 2 * kn) // 2
        part = nrm[c][...]
        q = lax.dot_general(wqkv[:cut, :], part, NT, preferred_element_type=F32)
        qkv = lax.dot_general(wqkv[cut:, :], part, NT, preferred_element_type=F32)
        qt[:cut, lo : lo + crow] = (q * 0.125).astype(BF16)
        qt[cut:, lo : lo + crow] = (qkv[: qn - cut] * 0.125).astype(BF16)
        kx[WINDOW + lo : WINDOW + lo + crow, :] = jnp.transpose(
            qkv[qn - cut : qn - cut + kn]
        ).astype(BF16)
        vt[:, WINDOW + lo : WINDOW + lo + crow] = qkv[qn - cut + kn :].astype(BF16)

    def tail_copy(n):
        src, dst = ((ktail, kin), (vtail, vin), (ptail, pin))[n]
        return pltpu.make_async_remote_copy(
            src_ref=src,
            dst_ref=dst,
            send_sem=tail_send.at[n],
            recv_sem=tail_recv.at[n],
            device_id={"sp": z + 1},
            device_id_type=MESH,
        )

    def tot_copy(d):
        return pltpu.make_async_remote_copy(
            src_ref=totout,
            dst_ref=totin.at[d - 1],
            send_sem=tot_send.at[d - 1],
            recv_sem=tot_recv.at[d - 1],
            device_id={"sp": z + d},
            device_id_type=MESH,
        )

    def carry_copy(d):
        return pltpu.make_async_remote_copy(
            src_ref=carryout,
            dst_ref=carryin,
            send_sem=carry_send.at[d - 1],
            recv_sem=carry_recv,
            device_id={"sp": z + d},
            device_id_type=MESH,
        )

    leads = (gi == GROUP - 1) & (z + 1 < nz)

    keyi = lax.broadcasted_iota(jnp.int32, (WINDOW, group * WINDOW), 0)
    posi = lax.broadcasted_iota(jnp.int32, (WINDOW, group * WINDOW), 1) & (WINDOW - 1)
    bi = lax.broadcasted_iota(jnp.int32, (WINDOW, 2 * WINDOW), 0)
    bj = lax.broadcasted_iota(jnp.int32, (WINDOW, 2 * WINDOW), 1)
    gap = bi + WINDOW - bj
    bands = [jnp.where((gap >= 0) & (gap < r), 1.0, 0.0).astype(BF16) for r in REACHES]
    bands.append(jnp.where((gap >= 0) & (bj >= WINDOW), 1.0, 0.0).astype(BF16))

    def counts(b):
        first = z * rows + b * WINDOW + 1
        return (lax.broadcasted_iota(jnp.int32, (WINDOW, 1), 0) + first).astype(F32)

    here = keyi <= posi
    masks[1] = jnp.where(here, 1.0, 0.0).astype(BF16)
    masks[0] = jnp.where(here, 0.0, 1.0).astype(BF16)

    def scores(n, b, h):
        lo = b * WINDOW
        qs = jnp.concatenate(
            [
                qt[64 * (group * h + j) : 64 * (group * h + j + 1), lo : lo + WINDOW]
                for j in range(group)
            ],
            axis=1,
        )
        blank = jnp.zeros_like(qs)
        qpad = jnp.concatenate([qs if i == h else blank for i in range(kv)], axis=0)
        s = jnp.dot(kx[lo : lo + 2 * WINDOW, :], qpad, preferred_element_type=F32)
        before = s[:WINDOW]
        if b == 0:
            before = before + jnp.where(z > 0, 0.0, NEG)
        sbuf[n] = jnp.where(here, s[WINDOW:], before)

    def weights(n, b, h):
        for j in range(0, group, 2):
            s = sbuf[n, :, j * WINDOW : (j + 2) * WINDOW]
            sink = jnp.concatenate(
                [jnp.full((1, WINDOW), sink_ref[group * h + j + i], F32) for i in range(2)], axis=1
            )
            top = jnp.maximum(jnp.max(s, axis=0, keepdims=True), sink)
            e = jnp.exp(s - top)
            tot = jnp.sum(e, axis=0, keepdims=True) + jnp.exp(sink - top)
            pbuf[n, :, j * WINDOW : (j + 2) * WINDOW] = (e * (1.0 / tot)).astype(BF16)

    def attend(n, b, h):
        lo = b * WINDOW
        w = pbuf[n]
        wt = jnp.concatenate([w * masks[0], w * masks[1]], axis=0)
        o = jnp.dot(
            vt[64 * h : 64 * (h + 1), lo : lo + 2 * WINDOW], wt, preferred_element_type=F32
        )
        o = jnp.concatenate([o[:, j * WINDOW : (j + 1) * WINDOW] for j in range(group)], axis=0)
        att[lo : lo + WINDOW, 64 * group * h : 64 * group * (h + 1)] = jnp.transpose(o).astype(BF16)

    def pool(b):
        spots = [n * WINDOW for n in (b, b + 1)]

        def both(g):
            return jnp.concatenate(
                [px[lo : lo + 2 * WINDOW, 128 * g : 128 * (g + 1)] for lo in spots], axis=1
            )

        means = []
        for g in range(3):
            near = both(g)
            sums = jnp.dot(bands[g], near, preferred_element_type=F32)
            here_in = near[WINDOW:].astype(F32)
            for n in range(2):
                part = slice(n * WINDOW, (n + 1) * WINDOW)
                scale = 1.0 / jnp.minimum(counts(b + n), float(REACHES[g]))
                means.append((sums[:, part] * scale - here_in[:, part]).astype(BF16))
        for n, lo in enumerate(spots):
            att[lo : lo + WINDOW, qn : qn + 256] = jnp.concatenate([means[n], means[2 + n]], axis=1)
            att[lo : lo + WINDOW, qn + 256 : qn + 384] = means[4 + n]
        sums = jnp.dot(bands[3], both(3), preferred_element_type=F32)
        for n, lo in enumerate(spots):
            l3[lo : lo + WINDOW, :] = sums[:, n * WINDOW : (n + 1) * WINDOW]

    def blocks(which, spots, beside):
        chains = [(b, h) for b in which for h in range(kv)]
        last = len(chains)
        beside = list(beside)
        for n in range(last + 6):
            if n < last:
                scores(n, *chains[n])
            if 0 <= n - 3 < last:
                weights(n - 3, *chains[n - 3])
            while spots and spots[0] == n:
                spots = spots[1:]
                step, *what = beside.pop(0)
                step(*what)
            if 0 <= n - 6 < last:
                attend(n - 6, *chains[n - 6])

    loads[6].wait()
    gain = gain_ref[...]

    @pl.when(me == 0)
    def _():
        tok_copy(2).wait()

    loads[0].wait()

    @pl.when(me == 0)
    def _():
        tok_copy(1).start()
        tok_copy(0).start()

    for load in loads[1:4]:
        load.start()
    for n in range(2):
        tok_send(n).wait_recv()
        norm(2, n * crow // 32, (n + 1) * crow // 32)
        for r in range(n * width // 256, (n + 1) * width // 256):
            sort_one(r)

    loads[4].start()
    loads[5].start()
    pool_in(2)

    @pl.when(me == 0)
    def _():
        tok_copy(1).wait()
        tok_copy(0).wait()

    tok_send(2).wait_recv()
    tok_send(3).wait_recv()
    for load in loads[1:4]:
        load.wait()
    norm(1)
    qkv_of(2)
    norm(0)
    qkv_of(1)

    ktail[...] = kx[rows : rows + WINDOW, :]
    vtail[...] = vt[:, rows : rows + WINDOW]
    ptail[...] = px[WINDOW + rows - TAIL : WINDOW + rows, 0:384]
    px[0:WINDOW, :] = jnp.zeros((WINDOW, px.shape[1]), BF16)
    kx[0:WINDOW, :] = jnp.zeros((WINDOW, kx.shape[1]), BF16)
    vt[:, 0:WINDOW] = jnp.zeros((vt.shape[0], WINDOW), BF16)

    @pl.when(z + 1 < nz)
    def _():
        pl.semaphore_wait(ready.at[0], 1)
        for n in range(3):
            tail_copy(n).start()

    loads[7].wait()

    blocks(range(nb - 1, nb // 2 - 1, -1), (1, 3, 5), ((pool_in, 1, 1), (qkv_of, 0), (pool_in, 0, 1)))

    total = jnp.sum(bt[0:nb, :], axis=0, keepdims=True)
    totout[...] = jnp.broadcast_to(total, totout.shape)
    for d in range(1, GROUP):

        @pl.when(gi + d < GROUP)
        def _():
            if d > 1:
                pl.semaphore_wait(ready.at[d - 1], 1)
            tot_copy(d).start()

    @pl.when(z > 0)
    def _():
        for n in range(3):
            tail_copy(n).wait_recv()
        kx[0:WINDOW, :] = kin[...]
        vt[:, 0:WINDOW] = vin[...]
        px[WINDOW - TAIL : WINDOW, 0:384] = pin[...]

    blocks(range(nb // 2 - 1, -1, -1), (5, 5, 9, 10, 11), ((pool_in, 1, 0), (pool_in, 0, 0), (pool, 4), (pool, 2), (pool, 0)))

    for d in range(1, GROUP):

        @pl.when(d <= gi)
        def _():
            tot_copy(d).wait_recv()

        @pl.when(d > gi)
        def _():
            totin[d - 1] = jnp.zeros(totin.shape[1:], F32)

    @pl.when(base > 0)
    def _():
        carry_copy(1).wait_recv()

    @pl.when(base == 0)
    def _():
        carryin[...] = jnp.zeros(carryin.shape, F32)

    carried = carryin[...]
    for d in range(1, GROUP):
        carried = carried + totin[d - 1]

    @pl.when(leads)
    def _():
        carryout[...] = carried + totout[...]
        for d in range(1, GROUP + 1):
            if d > 1:
                pl.semaphore_wait(ready.at[d - 1], 1)
            carry_copy(d).start()

    run = carried[0:1, :]
    for b in range(nb):
        lo = b * WINDOW
        mean = (l3[lo : lo + WINDOW, :] + run) * (1.0 / counts(b))
        run = run + bt[b : b + 1, :]
        att[lo : lo + WINDOW, qn + 384 :] = (
            mean - px[WINDOW + lo : WINDOW + lo + WINDOW, 384:].astype(F32)
        ).astype(BF16)

    orow = rows // 2
    ocol = width // OUT_CHUNKS
    for load in loads[4:6]:
        load.wait()

    def out_copy(n):
        cols = pl.ds(n * ocol, ocol)
        return pltpu.make_async_remote_copy(
            src_ref=sendbuf.at[:, cols],
            dst_ref=recvbuf.at[:, cols],
            send_sem=out_send.at[n],
            recv_sem=out_recv.at[n],
            device_id={"tp": other},
            device_id_type=MESH,
        )

    theirs = pl.ds(pl.multiple_of(other * orow, orow), orow)
    ours = pl.ds(pl.multiple_of(me * orow, orow), orow)
    for n in range(OUT_CHUNKS):
        cols = slice(n * ocol, (n + 1) * ocol)
        sendbuf[:, cols] = jnp.dot(
            att[theirs, :], wo[:, cols], preferred_element_type=F32
        ).astype(BF16)
        out_copy(n).start()
    def add(n):
        cols = slice(n * ocol, (n + 1) * ocol)
        outbuf[:, cols] = (own[n][...] + recvbuf[:, cols].astype(F32)).astype(BF16)

    for n in range(OUT_CHUNKS):
        cols = slice(n * ocol, (n + 1) * ocol)
        own[n][...] = jnp.dot(att[ours, :], wo[:, cols], preferred_element_type=F32)
    for n in range(OUT_CHUNKS):
        out_copy(n).wait_recv()
        add(n)

    for n in range(len(PARTS)):
        tok_send(n).wait_send()
    for d in range(1, GROUP):

        @pl.when(gi + d < GROUP)
        def _():
            tot_copy(d).wait_send()

    @pl.when(z + 1 < nz)
    def _():
        for n in range(3):
            tail_copy(n).wait_send()

    @pl.when(leads)
    def _():
        for d in range(1, GROUP + 1):
            carry_copy(d).wait_send()

    for n in range(OUT_CHUNKS):
        out_copy(n).wait_send()


def shards(
    tokens,
    norm_gain,
    query_weight,
    key_weight,
    value_weight,
    sink_logit,
    pool_weight,
    attn_out_weight,
    pool_out_weight,
):
    rows, half = tokens.shape[1:]
    width = 2 * half
    assert lax.axis_size("tp") == 2 and lax.axis_size("sp") % GROUP == 0
    turned = [
        jnp.transpose(w, (1, 2, 0)).reshape(-1, width)
        for w in (query_weight, key_weight, value_weight)
    ]
    qn, kn = turned[0].shape[0], turned[1].shape[0]
    pn = pool_weight.shape[1] * pool_weight.shape[2]
    wp = pool_weight.reshape(-1, pool_weight.shape[2])
    wa = attn_out_weight.reshape(-1, width)
    wpo = pool_out_weight.reshape(-1, width)
    anyspace = pl.BlockSpec(memory_space=pl.ANY)
    vm = pltpu.VMEM
    dma = pltpu.SemaphoreType.DMA
    orow = rows // 2
    out = pl.pallas_call(
        kernel,
        out_shape=pltpu.VMEM((orow, width), BF16),
        in_specs=[anyspace] * 9,
        out_specs=pl.BlockSpec(memory_space=pltpu.VMEM),
        scratch_shapes=[
            vm((rows, width), BF16),
            vm((rows // CHUNKS, width), BF16),
            vm((rows // CHUNKS, width), BF16),
            vm((rows // CHUNKS, width), BF16),
            vm((1, width), F32),
            pltpu.SMEM(sink_logit.shape, F32),
            vm((qn + 2 * kn, width), BF16),
            vm(wp.shape, BF16),
            vm((width, pn), BF16),
            vm((qn + pn, width), BF16),
            vm((qn, rows), BF16),
            vm((WINDOW + rows, kn), BF16),
            vm((kn, WINDOW + rows), BF16),
            vm((WINDOW + rows, pn), BF16),
            vm((rows, qn + pn), BF16),
            vm((rows, 128), F32),
            vm((8, 128), F32),
            vm((6, WINDOW, 512), F32),
            vm((6, WINDOW, 512), BF16),
            vm((2, WINDOW, 512), BF16),
            vm((WINDOW, kn), BF16),
            vm((kn, WINDOW), BF16),
            vm((TAIL, 384), BF16),
            vm((WINDOW, kn), BF16),
            vm((kn, WINDOW), BF16),
            vm((TAIL, 384), BF16),
            vm((8, 128), F32),
            vm((GROUP - 1, 8, 128), F32),
            vm((8, 128), F32),
            vm((8, 128), F32),
            vm((orow, width // OUT_CHUNKS), F32),
            vm((orow, width // OUT_CHUNKS), F32),
            vm((orow, width), BF16),
            vm((orow, width), BF16),
            dma((CHUNKS,)),
            dma((8,)),
            dma((len(PARTS),)),
            dma((len(PARTS),)),
            dma((3,)),
            dma((3,)),
            dma((GROUP - 1,)),
            dma((GROUP - 1,)),
            dma((GROUP,)),
            dma(()),
            dma((OUT_CHUNKS,)),
            dma((OUT_CHUNKS,)),
            pltpu.SemaphoreType.REGULAR((GROUP,)),
        ],
        compiler_params=pltpu.CompilerParams(
            collective_id=0, has_side_effects=True, vmem_limit_bytes=60 * 1024 * 1024
        ),
    )(tokens, norm_gain.reshape(1, width), *turned, sink_logit, wp, wa, wpo)
    return out[None]


def solution(mesh):
    in_specs = (
        P("fs", ("grp", "sp"), "tp"),
        P(),
        P(None, "tp", None),
        P(None, "tp", None),
        P(None, "tp", None),
        P("tp"),
        P(None, None, "tp"),
        P("tp", None, None),
        P(None, "tp", None),
    )
    out_specs = P("fs", ("grp", "sp", "tp"), None)
    return jax.shard_map(shards, mesh=mesh, in_specs=in_specs, out_specs=out_specs, check_vma=False)
```

```python
import functools

import jax
import jax.numpy as jnp
from jax import lax
from jax.experimental import pallas as pl
from jax.experimental.pallas import tpu as pltpu
from jax.sharding import PartitionSpec as P

WINDOW = 128
REACHES = (2, 4, 16)
TAIL = 16
GROUP = 4
CHUNKS = 3
PARTS = ((4, 1), (5, 1), (2, 2), (0, 2))
OUT_CHUNKS = 2
NEG = -1e30
BF16 = jnp.bfloat16
F32 = jnp.float32
MESH = pl.DeviceIdType.MESH
NT = (((1,), (1,)), ((), ()))


def kernel(
    tok_hbm, gain_hbm, wq_hbm, wk_hbm, wv_hbm, sink_hbm, wp_hbm, wa_hbm, wpo_hbm,
    outbuf,
    tok, nrm0, nrm1, nrm2, gain_ref, sink_ref, wqkv, wpraw, wp, wo, qt, kx, vt, px, att, l3, bt,
    sbuf, pbuf, masks,
    kin, vin, pin, ktail, vtail, ptail, totout, totin, carryout, carryin,
    own0, own1, sendbuf, recvbuf,
    tok_sem, w_sem, tsend, trecv, tail_send, tail_recv, tot_send, tot_recv,
    carry_send, carry_recv, out_send, out_recv, ready,
):
    me = lax.axis_index("tp")
    other = 1 - me
    z = lax.axis_index("sp")
    nz = lax.axis_size("sp")
    rows, width = tok.shape
    nrm = (nrm0, nrm1, nrm2)
    own = (own0, own1)
    half = width // 2
    heads = qt.shape[0] // 64
    kv = kx.shape[1] // 64
    group = heads // kv
    nb = rows // WINDOW
    crow = rows // CHUNKS
    gi = lax.rem(z, GROUP)
    base = z - gi

    mine = pl.ds(pl.multiple_of(me * half, half), half)

    def tok_copy(c):
        return pltpu.make_async_copy(
            tok_hbm.at[0, pl.ds(c * crow, crow), :],
            tok.at[pl.ds(c * crow, crow), mine],
            tok_sem.at[c],
        )

    qn, kn = wq_hbm.shape[0], wk_hbm.shape[0]
    class Split:
        def __init__(self, src, dst, low, pieces, first):
            step = src.shape[0] // pieces
            self.copies = [
                pltpu.make_async_copy(
                    src.at[pl.ds(n * step, step)],
                    dst.at[pl.ds(low + n * step, step)],
                    w_sem.at[first + n],
                )
                for n in range(pieces)
            ]

        def start(self):
            for copy in self.copies:
                copy.start()

        def wait(self):
            for copy in self.copies:
                copy.wait()

    loads = [
        Split(wp_hbm, wpraw, 0, 8, 0),
        Split(wq_hbm, wqkv, 0, 4, 8),
        Split(wk_hbm, wqkv, qn, 1, 12),
        Split(wv_hbm, wqkv, qn + kn, 1, 13),
        Split(wa_hbm, wo, 0, 1, 14),
        Split(wpo_hbm, wo, qn, 1, 15),
        pltpu.make_async_copy(gain_hbm, gain_ref, w_sem.at[16]),
        pltpu.make_async_copy(sink_hbm, sink_ref, w_sem.at[17]),
    ]
    barrier = pltpu.get_barrier_semaphore()
    pl.semaphore_signal(barrier, inc=1, device_id={"tp": other}, device_id_type=MESH)
    tok_copy(2).start()
    for load in (*loads[6:], loads[0]):
        load.start()

    @pl.when(me == 1)
    def _():
        tok_copy(1).start()
        tok_copy(0).start()


    def sends_to(d):
        inside = gi + d < GROUP
        leads = gi == GROUP - 1
        return (inside | leads) & (z + d < nz) if d < GROUP else leads & (z + d < nz)

    def hears_from(d):
        return (d <= gi) | ((d == gi + 1) & (base > 0))

    for d in range(1, GROUP + 1):

        @pl.when(sends_to(d))
        def _():
            pl.semaphore_signal(barrier, inc=1, device_id={"sp": z + d}, device_id_type=MESH)

    behind = gi + jnp.where(base > 0, 1, 0)
    pl.semaphore_wait(barrier, 1 + behind)

    def tok_send(n, loaded=False):
        first, count = PARTS[n]
        spot = pl.ds(first * WINDOW, count * WINDOW)
        return pltpu.make_async_remote_copy(
            src_ref=tok.at[spot, mine] if loaded else tok_hbm.at[0, spot, :],
            dst_ref=tok.at[spot, mine],
            send_sem=tsend.at[n],
            recv_sem=trecv.at[n],
            device_id={"tp": other},
            device_id_type=MESH,
        )

    @pl.when(me == 0)
    def _():
        for n in range(len(PARTS)):
            tok_send(n).start()

    @pl.when(me == 1)
    def _():
        for c in reversed(range(CHUNKS)):
            tok_copy(c).wait()
        for n in range(len(PARTS)):
            tok_send(n, True).start()

    for d in range(1, GROUP + 1):

        @pl.when(hears_from(d))
        def _():
            pl.semaphore_signal(ready.at[d - 1], inc=1, device_id={"sp": z - d}, device_id_type=MESH)

    pi = lax.broadcasted_iota(jnp.int32, (256, 256), 0)
    pc = lax.broadcasted_iota(jnp.int32, (256, 256), 1)
    perm = jnp.where(pc == 4 * (pi & 63) + (pi >> 6), 1.0, 0.0).astype(BF16)

    def sort_one(r):
        at = pl.multiple_of(r * 512, 512)
        pair = jnp.concatenate(
            [wpraw[pl.ds(at, 256), :], wpraw[pl.ds(at + 256, 256), :]], axis=1
        )
        got = jnp.dot(perm, pair, preferred_element_type=F32).astype(BF16)
        to = pl.multiple_of(r * 128, 128)
        for g in range(4):
            for s in range(2):
                wp[pl.ds(to + 64 * s, 64), pl.ds(128 * g, 128)] = got[
                    64 * g : 64 * g + 64, 128 * s : 128 * s + 128
                ]

    def norm(c, low=0, high=crow // 16):
        for n in range(low, high):
            x = tok[c * crow + 16 * n : c * crow + 16 * (n + 1), :].astype(F32)
            mean = jnp.sum(x * x, axis=1, keepdims=True) * (1.0 / width)
            scale = lax.rsqrt(mean + 1e-06)
            nrm[c][16 * n : 16 * (n + 1), :] = (x * scale * gain).astype(BF16)

    def pool_in(c, part=None):
        lo = c * crow
        for p in (0, 1) if part is None else (part,):
            cols = slice(256 * p, 256 * (p + 1))
            pooled_in = jnp.dot(nrm[c][...], wp[:, cols], preferred_element_type=F32).astype(BF16)
            px[WINDOW + lo : WINDOW + lo + crow, cols] = pooled_in
            if p == 1:
                for b in range(crow // WINDOW):
                    piece = pooled_in[b * WINDOW : (b + 1) * WINDOW, 128:].astype(F32)
                    n = c * (crow // WINDOW) + b
                    bt[n : n + 1, :] = jnp.sum(piece, axis=0, keepdims=True)

    def qkv_of(c):
        lo = c * crow
        cut = (qn + 2 * kn) // 2
        part = nrm[c][...]
        q = lax.dot_general(wqkv[:cut, :], part, NT, preferred_element_type=F32)
        qkv = lax.dot_general(wqkv[cut:, :], part, NT, preferred_element_type=F32)
        qt[:cut, lo : lo + crow] = (q * 0.125).astype(BF16)
        qt[cut:, lo : lo + crow] = (qkv[: qn - cut] * 0.125).astype(BF16)
        kx[WINDOW + lo : WINDOW + lo + crow, :] = jnp.transpose(
            qkv[qn - cut : qn - cut + kn]
        ).astype(BF16)
        vt[:, WINDOW + lo : WINDOW + lo + crow] = qkv[qn - cut + kn :].astype(BF16)

    def tail_copy(n):
        src, dst = ((ktail, kin), (vtail, vin), (ptail, pin))[n]
        return pltpu.make_async_remote_copy(
            src_ref=src,
            dst_ref=dst,
            send_sem=tail_send.at[n],
            recv_sem=tail_recv.at[n],
            device_id={"sp": z + 1},
            device_id_type=MESH,
        )

    def tot_copy(d):
        return pltpu.make_async_remote_copy(
            src_ref=totout,
            dst_ref=totin.at[d - 1],
            send_sem=tot_send.at[d - 1],
            recv_sem=tot_recv.at[d - 1],
            device_id={"sp": z + d},
            device_id_type=MESH,
        )

    def carry_copy(d):
        return pltpu.make_async_remote_copy(
            src_ref=carryout,
            dst_ref=carryin,
            send_sem=carry_send.at[d - 1],
            recv_sem=carry_recv,
            device_id={"sp": z + d},
            device_id_type=MESH,
        )

    leads = (gi == GROUP - 1) & (z + 1 < nz)

    keyi = lax.broadcasted_iota(jnp.int32, (WINDOW, group * WINDOW), 0)
    posi = lax.broadcasted_iota(jnp.int32, (WINDOW, group * WINDOW), 1) & (WINDOW - 1)
    bi = lax.broadcasted_iota(jnp.int32, (WINDOW, 2 * WINDOW), 0)
    bj = lax.broadcasted_iota(jnp.int32, (WINDOW, 2 * WINDOW), 1)
    gap = bi + WINDOW - bj
    bands = [jnp.where((gap >= 0) & (gap < r), 1.0, 0.0).astype(BF16) for r in REACHES]
    bands.append(jnp.where((gap >= 0) & (bj >= WINDOW), 1.0, 0.0).astype(BF16))

    def counts(b):
        first = z * rows + b * WINDOW + 1
        return (lax.broadcasted_iota(jnp.int32, (WINDOW, 1), 0) + first).astype(F32)

    here = keyi <= posi
    masks[1] = jnp.where(here, 1.0, 0.0).astype(BF16)
    masks[0] = jnp.where(here, 0.0, 1.0).astype(BF16)

    def scores(n, b, h):
        lo = b * WINDOW
        qs = jnp.concatenate(
            [
                qt[64 * (group * h + j) : 64 * (group * h + j + 1), lo : lo + WINDOW]
                for j in range(group)
            ],
            axis=1,
        )
        blank = jnp.zeros_like(qs)
        qpad = jnp.concatenate([qs if i == h else blank for i in range(kv)], axis=0)
        s = jnp.dot(kx[lo : lo + 2 * WINDOW, :], qpad, preferred_element_type=F32)
        before = s[:WINDOW]
        if b == 0:
            before = before + jnp.where(z > 0, 0.0, NEG)
        sbuf[n] = jnp.where(here, s[WINDOW:], before)

    def weights(n, b, h):
        for j in range(0, group, 2):
            s = sbuf[n, :, j * WINDOW : (j + 2) * WINDOW]
            sink = jnp.concatenate(
                [jnp.full((1, WINDOW), sink_ref[group * h + j + i], F32) for i in range(2)], axis=1
            )
            top = jnp.maximum(jnp.max(s, axis=0, keepdims=True), sink)
            e = jnp.exp(s - top)
            tot = jnp.sum(e, axis=0, keepdims=True) + jnp.exp(sink - top)
            pbuf[n, :, j * WINDOW : (j + 2) * WINDOW] = (e * (1.0 / tot)).astype(BF16)

    def attend(n, b, h):
        lo = b * WINDOW
        w = pbuf[n]
        wt = jnp.concatenate([w * masks[0], w * masks[1]], axis=0)
        o = jnp.dot(
            vt[64 * h : 64 * (h + 1), lo : lo + 2 * WINDOW], wt, preferred_element_type=F32
        )
        o = jnp.concatenate([o[:, j * WINDOW : (j + 1) * WINDOW] for j in range(group)], axis=0)
        att[lo : lo + WINDOW, 64 * group * h : 64 * group * (h + 1)] = jnp.transpose(o).astype(BF16)

    def pool(b):
        spots = [n * WINDOW for n in (b, b + 1)]

        def both(g):
            return jnp.concatenate(
                [px[lo : lo + 2 * WINDOW, 128 * g : 128 * (g + 1)] for lo in spots], axis=1
            )

        means = []
        for g in range(3):
            near = both(g)
            sums = jnp.dot(bands[g], near, preferred_element_type=F32)
            here_in = near[WINDOW:].astype(F32)
            for n in range(2):
                part = slice(n * WINDOW, (n + 1) * WINDOW)
                scale = 1.0 / jnp.minimum(counts(b + n), float(REACHES[g]))
                means.append((sums[:, part] * scale - here_in[:, part]).astype(BF16))
        for n, lo in enumerate(spots):
            att[lo : lo + WINDOW, qn : qn + 256] = jnp.concatenate([means[n], means[2 + n]], axis=1)
            att[lo : lo + WINDOW, qn + 256 : qn + 384] = means[4 + n]
        sums = jnp.dot(bands[3], both(3), preferred_element_type=F32)
        for n, lo in enumerate(spots):
            l3[lo : lo + WINDOW, :] = sums[:, n * WINDOW : (n + 1) * WINDOW]

    def blocks(which, spots, beside):
        chains = [(b, h) for b in which for h in range(kv)]
        last = len(chains)
        beside = list(beside)
        for n in range(last + 6):
            if n < last:
                scores(n, *chains[n])
            if 0 <= n - 3 < last:
                weights(n - 3, *chains[n - 3])
            while spots and spots[0] == n:
                spots = spots[1:]
                step, *what = beside.pop(0)
                step(*what)
            if 0 <= n - 6 < last:
                attend(n - 6, *chains[n - 6])

    loads[6].wait()
    gain = gain_ref[...]
    for load in loads[1:4]:
        load.start()

    @pl.when(me == 0)
    def _():
        tok_copy(2).wait()
        tok_copy(1).start()
        tok_copy(0).start()

    loads[0].wait()
    for n in range(2):
        tok_send(n).wait_recv()
        norm(2, n * crow // 32, (n + 1) * crow // 32)
        for r in range(n * width // 256, (n + 1) * width // 256):
            sort_one(r)

    loads[4].start()
    loads[5].start()
    pool_in(2)

    @pl.when(me == 0)
    def _():
        tok_copy(1).wait()
        tok_copy(0).wait()

    tok_send(2).wait_recv()
    tok_send(3).wait_recv()
    for load in loads[1:4]:
        load.wait()
    norm(1)
    qkv_of(2)
    norm(0)
    qkv_of(1)

    ktail[...] = kx[rows : rows + WINDOW, :]
    vtail[...] = vt[:, rows : rows + WINDOW]
    ptail[...] = px[WINDOW + rows - TAIL : WINDOW + rows, 0:384]
    px[0:WINDOW, :] = jnp.zeros((WINDOW, px.shape[1]), BF16)
    kx[0:WINDOW, :] = jnp.zeros((WINDOW, kx.shape[1]), BF16)
    vt[:, 0:WINDOW] = jnp.zeros((vt.shape[0], WINDOW), BF16)

    @pl.when(z + 1 < nz)
    def _():
        pl.semaphore_wait(ready.at[0], 1)
        for n in range(3):
            tail_copy(n).start()

    loads[7].wait()

    blocks(range(nb - 1, nb // 2 - 1, -1), (1, 3, 5), ((pool_in, 1, 1), (qkv_of, 0), (pool_in, 0, 1)))

    total = jnp.sum(bt[0:nb, :], axis=0, keepdims=True)
    totout[...] = jnp.broadcast_to(total, totout.shape)
    for d in range(1, GROUP):

        @pl.when(gi + d < GROUP)
        def _():
            if d > 1:
                pl.semaphore_wait(ready.at[d - 1], 1)
            tot_copy(d).start()

    @pl.when(z > 0)
    def _():
        for n in range(3):
            tail_copy(n).wait_recv()
        kx[0:WINDOW, :] = kin[...]
        vt[:, 0:WINDOW] = vin[...]
        px[WINDOW - TAIL : WINDOW, 0:384] = pin[...]

    blocks(range(nb // 2 - 1, -1, -1), (5, 5, 9, 10, 11), ((pool_in, 1, 0), (pool_in, 0, 0), (pool, 4), (pool, 2), (pool, 0)))

    for d in range(1, GROUP):

        @pl.when(d <= gi)
        def _():
            tot_copy(d).wait_recv()

        @pl.when(d > gi)
        def _():
            totin[d - 1] = jnp.zeros(totin.shape[1:], F32)

    @pl.when(base > 0)
    def _():
        carry_copy(1).wait_recv()

    @pl.when(base == 0)
    def _():
        carryin[...] = jnp.zeros(carryin.shape, F32)

    carried = carryin[...]
    for d in range(1, GROUP):
        carried = carried + totin[d - 1]

    @pl.when(leads)
    def _():
        carryout[...] = carried + totout[...]
        for d in range(1, GROUP + 1):
            if d > 1:
                pl.semaphore_wait(ready.at[d - 1], 1)
            carry_copy(d).start()

    run = carried[0:1, :]
    for b in range(nb):
        lo = b * WINDOW
        mean = (l3[lo : lo + WINDOW, :] + run) * (1.0 / counts(b))
        run = run + bt[b : b + 1, :]
        att[lo : lo + WINDOW, qn + 384 :] = (
            mean - px[WINDOW + lo : WINDOW + lo + WINDOW, 384:].astype(F32)
        ).astype(BF16)

    orow = rows // 2
    ocol = width // OUT_CHUNKS
    for load in loads[4:6]:
        load.wait()

    def out_copy(n):
        cols = pl.ds(n * ocol, ocol)
        return pltpu.make_async_remote_copy(
            src_ref=sendbuf.at[:, cols],
            dst_ref=recvbuf.at[:, cols],
            send_sem=out_send.at[n],
            recv_sem=out_recv.at[n],
            device_id={"tp": other},
            device_id_type=MESH,
        )

    theirs = pl.ds(pl.multiple_of(other * orow, orow), orow)
    ours = pl.ds(pl.multiple_of(me * orow, orow), orow)
    for n in range(OUT_CHUNKS):
        cols = slice(n * ocol, (n + 1) * ocol)
        sendbuf[:, cols] = jnp.dot(
            att[theirs, :], wo[:, cols], preferred_element_type=F32
        ).astype(BF16)
        out_copy(n).start()
    def add(n):
        cols = slice(n * ocol, (n + 1) * ocol)
        outbuf[:, cols] = (own[n][...] + recvbuf[:, cols].astype(F32)).astype(BF16)

    for n in range(OUT_CHUNKS):
        cols = slice(n * ocol, (n + 1) * ocol)
        own[n][...] = jnp.dot(att[ours, :], wo[:, cols], preferred_element_type=F32)
    for n in range(OUT_CHUNKS):
        out_copy(n).wait_recv()
        add(n)

    for n in range(len(PARTS)):
        tok_send(n).wait_send()
    for d in range(1, GROUP):

        @pl.when(gi + d < GROUP)
        def _():
            tot_copy(d).wait_send()

    @pl.when(z + 1 < nz)
    def _():
        for n in range(3):
            tail_copy(n).wait_send()

    @pl.when(leads)
    def _():
        for d in range(1, GROUP + 1):
            carry_copy(d).wait_send()

    for n in range(OUT_CHUNKS):
        out_copy(n).wait_send()


def shards(
    tokens,
    norm_gain,
    query_weight,
    key_weight,
    value_weight,
    sink_logit,
    pool_weight,
    attn_out_weight,
    pool_out_weight,
):
    rows, half = tokens.shape[1:]
    width = 2 * half
    assert lax.axis_size("tp") == 2 and lax.axis_size("sp") % GROUP == 0
    turned = [
        jnp.transpose(w, (1, 2, 0)).reshape(-1, width)
        for w in (query_weight, key_weight, value_weight)
    ]
    qn, kn = turned[0].shape[0], turned[1].shape[0]
    pn = pool_weight.shape[1] * pool_weight.shape[2]
    wp = pool_weight.reshape(-1, pool_weight.shape[2])
    wa = attn_out_weight.reshape(-1, width)
    wpo = pool_out_weight.reshape(-1, width)
    anyspace = pl.BlockSpec(memory_space=pl.ANY)
    vm = pltpu.VMEM
    dma = pltpu.SemaphoreType.DMA
    orow = rows // 2
    out = pl.pallas_call(
        kernel,
        out_shape=pltpu.VMEM((orow, width), BF16),
        in_specs=[anyspace] * 9,
        out_specs=pl.BlockSpec(memory_space=pltpu.VMEM),
        scratch_shapes=[
            vm((rows, width), BF16),
            vm((rows // CHUNKS, width), BF16),
            vm((rows // CHUNKS, width), BF16),
            vm((rows // CHUNKS, width), BF16),
            vm((1, width), F32),
            pltpu.SMEM(sink_logit.shape, F32),
            vm((qn + 2 * kn, width), BF16),
            vm(wp.shape, BF16),
            vm((width, pn), BF16),
            vm((qn + pn, width), BF16),
            vm((qn, rows), BF16),
            vm((WINDOW + rows, kn), BF16),
            vm((kn, WINDOW + rows), BF16),
            vm((WINDOW + rows, pn), BF16),
            vm((rows, qn + pn), BF16),
            vm((rows, 128), F32),
            vm((8, 128), F32),
            vm((6, WINDOW, 512), F32),
            vm((6, WINDOW, 512), BF16),
            vm((2, WINDOW, 512), BF16),
            vm((WINDOW, kn), BF16),
            vm((kn, WINDOW), BF16),
            vm((TAIL, 384), BF16),
            vm((WINDOW, kn), BF16),
            vm((kn, WINDOW), BF16),
            vm((TAIL, 384), BF16),
            vm((8, 128), F32),
            vm((GROUP - 1, 8, 128), F32),
            vm((8, 128), F32),
            vm((8, 128), F32),
            vm((orow, width // OUT_CHUNKS), F32),
            vm((orow, width // OUT_CHUNKS), F32),
            vm((orow, width), BF16),
            vm((orow, width), BF16),
            dma((CHUNKS,)),
            dma((18,)),
            dma((len(PARTS),)),
            dma((len(PARTS),)),
            dma((3,)),
            dma((3,)),
            dma((GROUP - 1,)),
            dma((GROUP - 1,)),
            dma((GROUP,)),
            dma(()),
            dma((OUT_CHUNKS,)),
            dma((OUT_CHUNKS,)),
            pltpu.SemaphoreType.REGULAR((GROUP,)),
        ],
        compiler_params=pltpu.CompilerParams(
            collective_id=0, has_side_effects=True, vmem_limit_bytes=60 * 1024 * 1024
        ),
    )(tokens, norm_gain.reshape(1, width), *turned, sink_logit, wp, wa, wpo)
    return out[None]


def solution(mesh):
    in_specs = (
        P("fs", ("grp", "sp"), "tp"),
        P(),
        P(None, "tp", None),
        P(None, "tp", None),
        P(None, "tp", None),
        P("tp"),
        P(None, None, "tp"),
        P("tp", None, None),
        P(None, "tp", None),
    )
    out_specs = P("fs", ("grp", "sp", "tp"), None)
    return jax.shard_map(shards, mesh=mesh, in_specs=in_specs, out_specs=out_specs, check_vma=False)
```

```python
import functools

import jax
import jax.numpy as jnp
from jax import lax
from jax.experimental import pallas as pl
from jax.experimental.pallas import tpu as pltpu
from jax.sharding import PartitionSpec as P

WINDOW = 128
REACHES = (2, 4, 16)
TAIL = 16
GROUP = 4
CHUNKS = 3
PARTS = ((4, 1), (5, 1), (2, 2), (0, 2))
OUT_CHUNKS = 2
NEG = -1e30
BF16 = jnp.bfloat16
F32 = jnp.float32
MESH = pl.DeviceIdType.MESH
NT = (((1,), (1,)), ((), ()))


def kernel(
    tok_hbm, gain_hbm, wq_hbm, wk_hbm, wv_hbm, sink_hbm, wp_hbm, wa_hbm, wpo_hbm,
    outbuf,
    tok, nrm0, nrm1, nrm2, gain_ref, sink_ref, wqkv, wpraw, wp, wo, qt, kx, vt, px, att, l3, bt,
    sbuf, pbuf, masks,
    kin, vin, pin, ktail, vtail, ptail, totout, totin, carryout, carryin,
    own0, own1, sendbuf, recvbuf,
    tok_sem, w_sem, tsend, trecv, tail_send, tail_recv, tot_send, tot_recv,
    carry_send, carry_recv, out_send, out_recv, ready,
):
    me = lax.axis_index("tp")
    other = 1 - me
    z = lax.axis_index("sp")
    nz = lax.axis_size("sp")
    rows, width = tok.shape
    nrm = (nrm0, nrm1, nrm2)
    own = (own0, own1)
    half = width // 2
    heads = qt.shape[0] // 64
    kv = kx.shape[1] // 64
    group = heads // kv
    nb = rows // WINDOW
    crow = rows // CHUNKS
    gi = lax.rem(z, GROUP)
    base = z - gi

    mine = pl.ds(pl.multiple_of(me * half, half), half)

    def tok_copy(c):
        return pltpu.make_async_copy(
            tok_hbm.at[0, pl.ds(c * crow, crow), :],
            tok.at[pl.ds(c * crow, crow), mine],
            tok_sem.at[c],
        )

    qn, kn = wq_hbm.shape[0], wk_hbm.shape[0]
    class Split:
        def __init__(self, src, dst, low, pieces, first):
            step = src.shape[0] // pieces
            self.copies = [
                pltpu.make_async_copy(
                    src.at[pl.ds(n * step, step)],
                    dst.at[pl.ds(low + n * step, step)],
                    w_sem.at[first + n],
                )
                for n in range(pieces)
            ]

        def start(self):
            for copy in self.copies:
                copy.start()

        def wait(self):
            for copy in self.copies:
                copy.wait()

    loads = [
        Split(wp_hbm, wpraw, 0, 8, 0),
        Split(wq_hbm, wqkv, 0, 4, 8),
        Split(wk_hbm, wqkv, qn, 1, 12),
        Split(wv_hbm, wqkv, qn + kn, 1, 13),
        Split(wa_hbm, wo, 0, 1, 14),
        Split(wpo_hbm, wo, qn, 1, 15),
        pltpu.make_async_copy(gain_hbm, gain_ref, w_sem.at[16]),
        pltpu.make_async_copy(sink_hbm, sink_ref, w_sem.at[17]),
    ]
    barrier = pltpu.get_barrier_semaphore()
    pl.semaphore_signal(barrier, inc=1, device_id={"tp": other}, device_id_type=MESH)
    tok_copy(2).start()
    for load in (*loads[6:], loads[0]):
        load.start()

    @pl.when(me == 1)
    def _():
        tok_copy(1).start()
        tok_copy(0).start()


    def sends_to(d):
        inside = gi + d < GROUP
        leads = gi == GROUP - 1
        return (inside | leads) & (z + d < nz) if d < GROUP else leads & (z + d < nz)

    def hears_from(d):
        return (d <= gi) | ((d == gi + 1) & (base > 0))

    for d in range(1, GROUP + 1):

        @pl.when(sends_to(d))
        def _():
            pl.semaphore_signal(barrier, inc=1, device_id={"sp": z + d}, device_id_type=MESH)

    behind = gi + jnp.where(base > 0, 1, 0)
    pl.semaphore_wait(barrier, 1 + behind)

    def tok_send(n, loaded=False):
        first, count = PARTS[n]
        spot = pl.ds(first * WINDOW, count * WINDOW)
        return pltpu.make_async_remote_copy(
            src_ref=tok.at[spot, mine] if loaded else tok_hbm.at[0, spot, :],
            dst_ref=tok.at[spot, mine],
            send_sem=tsend.at[n],
            recv_sem=trecv.at[n],
            device_id={"tp": other},
            device_id_type=MESH,
        )

    @pl.when(me == 0)
    def _():
        for n in range(len(PARTS)):
            tok_send(n).start()

    @pl.when(me == 1)
    def _():
        for c in reversed(range(CHUNKS)):
            tok_copy(c).wait()
        for n in range(len(PARTS)):
            tok_send(n, True).start()

    for d in range(1, GROUP + 1):

        @pl.when(hears_from(d))
        def _():
            pl.semaphore_signal(ready.at[d - 1], inc=1, device_id={"sp": z - d}, device_id_type=MESH)

    pi = lax.broadcasted_iota(jnp.int32, (256, 256), 0)
    pc = lax.broadcasted_iota(jnp.int32, (256, 256), 1)
    perm = jnp.where(pc == 4 * (pi & 63) + (pi >> 6), 1.0, 0.0).astype(BF16)

    def sort_one(r):
        at = pl.multiple_of(r * 512, 512)
        pair = jnp.concatenate(
            [wpraw[pl.ds(at, 256), :], wpraw[pl.ds(at + 256, 256), :]], axis=1
        )
        got = jnp.dot(perm, pair, preferred_element_type=F32).astype(BF16)
        to = pl.multiple_of(r * 128, 128)
        for g in range(4):
            for s in range(2):
                wp[pl.ds(to + 64 * s, 64), pl.ds(128 * g, 128)] = got[
                    64 * g : 64 * g + 64, 128 * s : 128 * s + 128
                ]

    def norm(c, low=0, high=crow // 16):
        for n in range(low, high):
            x = tok[c * crow + 16 * n : c * crow + 16 * (n + 1), :].astype(F32)
            mean = jnp.sum(x * x, axis=1, keepdims=True) * (1.0 / width)
            scale = lax.rsqrt(mean + 1e-06)
            nrm[c][16 * n : 16 * (n + 1), :] = (x * scale * gain).astype(BF16)

    def pool_in(c, part=None):
        lo = c * crow
        for p in (0, 1) if part is None else (part,):
            cols = slice(256 * p, 256 * (p + 1))
            pooled_in = jnp.dot(nrm[c][...], wp[:, cols], preferred_element_type=F32).astype(BF16)
            px[WINDOW + lo : WINDOW + lo + crow, cols] = pooled_in
            if p == 1:
                for b in range(crow // WINDOW):
                    piece = pooled_in[b * WINDOW : (b + 1) * WINDOW, 128:].astype(F32)
                    n = c * (crow // WINDOW) + b
                    bt[n : n + 1, :] = jnp.sum(piece, axis=0, keepdims=True)

    def qkv_of(c):
        lo = c * crow
        cut = (qn + 2 * kn) // 2
        part = nrm[c][...]
        q = lax.dot_general(wqkv[:cut, :], part, NT, preferred_element_type=F32)
        qkv = lax.dot_general(wqkv[cut:, :], part, NT, preferred_element_type=F32)
        qt[:cut, lo : lo + crow] = (q * 0.125).astype(BF16)
        qt[cut:, lo : lo + crow] = (qkv[: qn - cut] * 0.125).astype(BF16)
        kx[WINDOW + lo : WINDOW + lo + crow, :] = jnp.transpose(
            qkv[qn - cut : qn - cut + kn]
        ).astype(BF16)
        vt[:, WINDOW + lo : WINDOW + lo + crow] = qkv[qn - cut + kn :].astype(BF16)

    def tail_copy(n):
        src, dst = ((ktail, kin), (vtail, vin), (ptail, pin))[n]
        return pltpu.make_async_remote_copy(
            src_ref=src,
            dst_ref=dst,
            send_sem=tail_send.at[n],
            recv_sem=tail_recv.at[n],
            device_id={"sp": z + 1},
            device_id_type=MESH,
        )

    def tot_copy(d):
        return pltpu.make_async_remote_copy(
            src_ref=totout,
            dst_ref=totin.at[d - 1],
            send_sem=tot_send.at[d - 1],
            recv_sem=tot_recv.at[d - 1],
            device_id={"sp": z + d},
            device_id_type=MESH,
        )

    def carry_copy(d):
        return pltpu.make_async_remote_copy(
            src_ref=carryout,
            dst_ref=carryin,
            send_sem=carry_send.at[d - 1],
            recv_sem=carry_recv,
            device_id={"sp": z + d},
            device_id_type=MESH,
        )

    leads = (gi == GROUP - 1) & (z + 1 < nz)

    keyi = lax.broadcasted_iota(jnp.int32, (WINDOW, group * WINDOW), 0)
    posi = lax.broadcasted_iota(jnp.int32, (WINDOW, group * WINDOW), 1) & (WINDOW - 1)
    bi = lax.broadcasted_iota(jnp.int32, (WINDOW, 2 * WINDOW), 0)
    bj = lax.broadcasted_iota(jnp.int32, (WINDOW, 2 * WINDOW), 1)
    gap = bi + WINDOW - bj
    bands = [jnp.where((gap >= 0) & (gap < r), 1.0, 0.0).astype(BF16) for r in REACHES]
    bands.append(jnp.where((gap >= 0) & (bj >= WINDOW), 1.0, 0.0).astype(BF16))

    def counts(b):
        first = z * rows + b * WINDOW + 1
        return (lax.broadcasted_iota(jnp.int32, (WINDOW, 1), 0) + first).astype(F32)

    here = keyi <= posi
    masks[1] = jnp.where(here, 1.0, 0.0).astype(BF16)
    masks[0] = jnp.where(here, 0.0, 1.0).astype(BF16)

    def scores(n, b, h):
        lo = b * WINDOW
        qs = jnp.concatenate(
            [
                qt[64 * (group * h + j) : 64 * (group * h + j + 1), lo : lo + WINDOW]
                for j in range(group)
            ],
            axis=1,
        )
        blank = jnp.zeros_like(qs)
        qpad = jnp.concatenate([qs if i == h else blank for i in range(kv)], axis=0)
        s = jnp.dot(kx[lo : lo + 2 * WINDOW, :], qpad, preferred_element_type=F32)
        before = s[:WINDOW]
        if b == 0:
            before = before + jnp.where(z > 0, 0.0, NEG)
        sbuf[n] = jnp.where(here, s[WINDOW:], before)

    def weights(n, b, h):
        for j in range(0, group, 2):
            s = sbuf[n, :, j * WINDOW : (j + 2) * WINDOW]
            sink = jnp.concatenate(
                [jnp.full((1, WINDOW), sink_ref[group * h + j + i], F32) for i in range(2)], axis=1
            )
            top = jnp.maximum(jnp.max(s, axis=0, keepdims=True), sink)
            e = jnp.exp(s - top)
            tot = jnp.sum(e, axis=0, keepdims=True) + jnp.exp(sink - top)
            pbuf[n, :, j * WINDOW : (j + 2) * WINDOW] = (e * (1.0 / tot)).astype(BF16)

    def attend(n, b, h):
        lo = b * WINDOW
        w = pbuf[n]
        wt = jnp.concatenate([w * masks[0], w * masks[1]], axis=0)
        o = jnp.dot(
            vt[64 * h : 64 * (h + 1), lo : lo + 2 * WINDOW], wt, preferred_element_type=F32
        )
        o = jnp.concatenate([o[:, j * WINDOW : (j + 1) * WINDOW] for j in range(group)], axis=0)
        att[lo : lo + WINDOW, 64 * group * h : 64 * group * (h + 1)] = jnp.transpose(o).astype(BF16)

    def pool(b):
        spots = [n * WINDOW for n in (b, b + 1)]

        def both(g):
            return jnp.concatenate(
                [px[lo : lo + 2 * WINDOW, 128 * g : 128 * (g + 1)] for lo in spots], axis=1
            )

        means = []
        for g in range(3):
            near = both(g)
            sums = jnp.dot(bands[g], near, preferred_element_type=F32)
            here_in = near[WINDOW:].astype(F32)
            for n in range(2):
                part = slice(n * WINDOW, (n + 1) * WINDOW)
                scale = 1.0 / jnp.minimum(counts(b + n), float(REACHES[g]))
                means.append((sums[:, part] * scale - here_in[:, part]).astype(BF16))
        for n, lo in enumerate(spots):
            att[lo : lo + WINDOW, qn : qn + 256] = jnp.concatenate([means[n], means[2 + n]], axis=1)
            att[lo : lo + WINDOW, qn + 256 : qn + 384] = means[4 + n]
        sums = jnp.dot(bands[3], both(3), preferred_element_type=F32)
        for n, lo in enumerate(spots):
            l3[lo : lo + WINDOW, :] = sums[:, n * WINDOW : (n + 1) * WINDOW]

    def blocks(which, spots, beside):
        chains = [(b, h) for b in which for h in range(kv)]
        last = len(chains)
        beside = list(beside)
        for n in range(last + 6):
            if n < last:
                scores(n, *chains[n])
            if 0 <= n - 3 < last:
                weights(n - 3, *chains[n - 3])
            while spots and spots[0] == n:
                spots = spots[1:]
                step, *what = beside.pop(0)
                step(*what)
            if 0 <= n - 6 < last:
                attend(n - 6, *chains[n - 6])

    loads[6].wait()
    gain = gain_ref[...]

    @pl.when(me == 0)
    def _():
        tok_copy(2).wait()

    for load in loads[1:4]:
        load.start()

    @pl.when(me == 0)
    def _():
        tok_copy(1).start()
        tok_copy(0).start()

    loads[0].wait()
    for n in range(2):
        tok_send(n).wait_recv()
        norm(2, n * crow // 32, (n + 1) * crow // 32)
        for r in range(n * width // 256, (n + 1) * width // 256):
            sort_one(r)

    loads[4].start()
    loads[5].start()
    pool_in(2)

    @pl.when(me == 0)
    def _():
        tok_copy(1).wait()
        tok_copy(0).wait()

    tok_send(2).wait_recv()
    tok_send(3).wait_recv()
    for load in loads[1:4]:
        load.wait()
    norm(1)
    qkv_of(2)
    norm(0)
    qkv_of(1)

    ktail[...] = kx[rows : rows + WINDOW, :]
    vtail[...] = vt[:, rows : rows + WINDOW]
    ptail[...] = px[WINDOW + rows - TAIL : WINDOW + rows, 0:384]
    px[0:WINDOW, :] = jnp.zeros((WINDOW, px.shape[1]), BF16)
    kx[0:WINDOW, :] = jnp.zeros((WINDOW, kx.shape[1]), BF16)
    vt[:, 0:WINDOW] = jnp.zeros((vt.shape[0], WINDOW), BF16)

    @pl.when(z + 1 < nz)
    def _():
        pl.semaphore_wait(ready.at[0], 1)
        for n in range(3):
            tail_copy(n).start()

    loads[7].wait()

    blocks(range(nb - 1, nb // 2 - 1, -1), (1, 3, 5), ((pool_in, 1, 1), (qkv_of, 0), (pool_in, 0, 1)))

    total = jnp.sum(bt[0:nb, :], axis=0, keepdims=True)
    totout[...] = jnp.broadcast_to(total, totout.shape)
    for d in range(1, GROUP):

        @pl.when(gi + d < GROUP)
        def _():
            if d > 1:
                pl.semaphore_wait(ready.at[d - 1], 1)
            tot_copy(d).start()

    @pl.when(z > 0)
    def _():
        for n in range(3):
            tail_copy(n).wait_recv()
        kx[0:WINDOW, :] = kin[...]
        vt[:, 0:WINDOW] = vin[...]
        px[WINDOW - TAIL : WINDOW, 0:384] = pin[...]

    blocks(range(nb // 2 - 1, -1, -1), (5, 5, 9, 10, 11), ((pool_in, 1, 0), (pool_in, 0, 0), (pool, 4), (pool, 2), (pool, 0)))

    for d in range(1, GROUP):

        @pl.when(d <= gi)
        def _():
            tot_copy(d).wait_recv()

        @pl.when(d > gi)
        def _():
            totin[d - 1] = jnp.zeros(totin.shape[1:], F32)

    @pl.when(base > 0)
    def _():
        carry_copy(1).wait_recv()

    @pl.when(base == 0)
    def _():
        carryin[...] = jnp.zeros(carryin.shape, F32)

    carried = carryin[...]
    for d in range(1, GROUP):
        carried = carried + totin[d - 1]

    @pl.when(leads)
    def _():
        carryout[...] = carried + totout[...]
        for d in range(1, GROUP + 1):
            if d > 1:
                pl.semaphore_wait(ready.at[d - 1], 1)
            carry_copy(d).start()

    run = carried[0:1, :]
    for b in range(nb):
        lo = b * WINDOW
        mean = (l3[lo : lo + WINDOW, :] + run) * (1.0 / counts(b))
        run = run + bt[b : b + 1, :]
        att[lo : lo + WINDOW, qn + 384 :] = (
            mean - px[WINDOW + lo : WINDOW + lo + WINDOW, 384:].astype(F32)
        ).astype(BF16)

    orow = rows // 2
    ocol = width // OUT_CHUNKS
    for load in loads[4:6]:
        load.wait()

    def out_copy(n):
        cols = pl.ds(n * ocol, ocol)
        return pltpu.make_async_remote_copy(
            src_ref=sendbuf.at[:, cols],
            dst_ref=recvbuf.at[:, cols],
            send_sem=out_send.at[n],
            recv_sem=out_recv.at[n],
            device_id={"tp": other},
            device_id_type=MESH,
        )

    theirs = pl.ds(pl.multiple_of(other * orow, orow), orow)
    ours = pl.ds(pl.multiple_of(me * orow, orow), orow)
    for n in range(OUT_CHUNKS):
        cols = slice(n * ocol, (n + 1) * ocol)
        sendbuf[:, cols] = jnp.dot(
            att[theirs, :], wo[:, cols], preferred_element_type=F32
        ).astype(BF16)
        out_copy(n).start()
    def add(n):
        cols = slice(n * ocol, (n + 1) * ocol)
        outbuf[:, cols] = (own[n][...] + recvbuf[:, cols].astype(F32)).astype(BF16)

    for n in range(OUT_CHUNKS):
        cols = slice(n * ocol, (n + 1) * ocol)
        own[n][...] = jnp.dot(att[ours, :], wo[:, cols], preferred_element_type=F32)
    for n in range(OUT_CHUNKS):
        out_copy(n).wait_recv()
        add(n)

    for n in range(len(PARTS)):
        tok_send(n).wait_send()
    for d in range(1, GROUP):

        @pl.when(gi + d < GROUP)
        def _():
            tot_copy(d).wait_send()

    @pl.when(z + 1 < nz)
    def _():
        for n in range(3):
            tail_copy(n).wait_send()

    @pl.when(leads)
    def _():
        for d in range(1, GROUP + 1):
            carry_copy(d).wait_send()

    for n in range(OUT_CHUNKS):
        out_copy(n).wait_send()


def shards(
    tokens,
    norm_gain,
    query_weight,
    key_weight,
    value_weight,
    sink_logit,
    pool_weight,
    attn_out_weight,
    pool_out_weight,
):
    rows, half = tokens.shape[1:]
    width = 2 * half
    assert lax.axis_size("tp") == 2 and lax.axis_size("sp") % GROUP == 0
    turned = [
        jnp.transpose(w, (1, 2, 0)).reshape(-1, width)
        for w in (query_weight, key_weight, value_weight)
    ]
    qn, kn = turned[0].shape[0], turned[1].shape[0]
    pn = pool_weight.shape[1] * pool_weight.shape[2]
    wp = pool_weight.reshape(-1, pool_weight.shape[2])
    wa = attn_out_weight.reshape(-1, width)
    wpo = pool_out_weight.reshape(-1, width)
    anyspace = pl.BlockSpec(memory_space=pl.ANY)
    vm = pltpu.VMEM
    dma = pltpu.SemaphoreType.DMA
    orow = rows // 2
    out = pl.pallas_call(
        kernel,
        out_shape=pltpu.VMEM((orow, width), BF16),
        in_specs=[anyspace] * 9,
        out_specs=pl.BlockSpec(memory_space=pltpu.VMEM),
        scratch_shapes=[
            vm((rows, width), BF16),
            vm((rows // CHUNKS, width), BF16),
            vm((rows // CHUNKS, width), BF16),
            vm((rows // CHUNKS, width), BF16),
            vm((1, width), F32),
            pltpu.SMEM(sink_logit.shape, F32),
            vm((qn + 2 * kn, width), BF16),
            vm(wp.shape, BF16),
            vm((width, pn), BF16),
            vm((qn + pn, width), BF16),
            vm((qn, rows), BF16),
            vm((WINDOW + rows, kn), BF16),
            vm((kn, WINDOW + rows), BF16),
            vm((WINDOW + rows, pn), BF16),
            vm((rows, qn + pn), BF16),
            vm((rows, 128), F32),
            vm((8, 128), F32),
            vm((6, WINDOW, 512), F32),
            vm((6, WINDOW, 512), BF16),
            vm((2, WINDOW, 512), BF16),
            vm((WINDOW, kn), BF16),
            vm((kn, WINDOW), BF16),
            vm((TAIL, 384), BF16),
            vm((WINDOW, kn), BF16),
            vm((kn, WINDOW), BF16),
            vm((TAIL, 384), BF16),
            vm((8, 128), F32),
            vm((GROUP - 1, 8, 128), F32),
            vm((8, 128), F32),
            vm((8, 128), F32),
            vm((orow, width // OUT_CHUNKS), F32),
            vm((orow, width // OUT_CHUNKS), F32),
            vm((orow, width), BF16),
            vm((orow, width), BF16),
            dma((CHUNKS,)),
            dma((18,)),
            dma((len(PARTS),)),
            dma((len(PARTS),)),
            dma((3,)),
            dma((3,)),
            dma((GROUP - 1,)),
            dma((GROUP - 1,)),
            dma((GROUP,)),
            dma(()),
            dma((OUT_CHUNKS,)),
            dma((OUT_CHUNKS,)),
            pltpu.SemaphoreType.REGULAR((GROUP,)),
        ],
        compiler_params=pltpu.CompilerParams(
            collective_id=0, has_side_effects=True, vmem_limit_bytes=60 * 1024 * 1024
        ),
    )(tokens, norm_gain.reshape(1, width), *turned, sink_logit, wp, wa, wpo)
    return out[None]


def solution(mesh):
    in_specs = (
        P("fs", ("grp", "sp"), "tp"),
        P(),
        P(None, "tp", None),
        P(None, "tp", None),
        P(None, "tp", None),
        P("tp"),
        P(None, None, "tp"),
        P("tp", None, None),
        P(None, "tp", None),
    )
    out_specs = P("fs", ("grp", "sp", "tp"), None)
    return jax.shard_map(shards, mesh=mesh, in_specs=in_specs, out_specs=out_specs, check_vma=False)
```
